512 devices in a mesh: sp: 128 (over z, x, core), tp: 4 (over y).
Axes of the slice: x: 4, y: 4, z: 16, core: 2. Of those that a mesh axis runs over, the one named last changes fastest.
Arguments:
- value_rows: bfloat16 [131072, 1024], P('sp', 'tp'), may hold values from -6 to 6
- gate_rows: bfloat16 [131072, 1024], P('sp', 'tp'), may hold values from -6 to 6
- conv_taps: bfloat16 [31, 1024], P(None, 'tp'), may hold values from -1 to 1
- norm_gain: float32 [1024], P('tp'), may hold values from 0.1 to 1.9
- point_weight: bfloat16 [1024, 1024], P(None, 'tp'), may hold values from -0.1875 to 0.1875
- out_grad: bfloat16 [131072, 1024], P('sp', 'tp'), may hold values from -24 to 24
Outputs:
- value_grad: bfloat16 [131072, 1024], P('sp', 'tp')
- gate_grad: bfloat16 [131072, 1024], P('sp', 'tp')
- taps_grad: float32 [31, 1024], P(None, 'tp')
- gain_grad: float32 [1024], P('tp')
- weight_grad: float32 [1024, 1024], P('sp', 'tp')
The draws below stay inside these ranges and needn't reach their ends.
All inputs are finite; a program needn't handle non-finite values.
Results may differ from the reference program's by a relative error of at most 0.0051.
Values may be sent and summed in bfloat16 or wider, within the bound.
No kernel may reach another device: no remote copies, remote signals or barrier semaphores. Data moves between devices by JAX's collectives and lax.ppermute only.
A program may use at most 128 MiB of HBM per device.

```python
import jax
import jax.numpy as jnp
from jax import lax

C = 1024
GROUP = 64
KW = 31
HALF = 15
TOK_DEV = 1024
TOKENS = 131072


def raised(array, key, source, target, blocks, factor):
    def block_of(dim):
        return (jnp.arange(array.shape[dim]) // (array.shape[dim] // blocks)).reshape((-1,) + (1,) * (array.ndim - 1 - dim))

    near = jax.random.permutation(key, blocks)[block_of(target)]
    second = (block_of(target) + blocks // 2) % blocks
    return jnp.where((block_of(source) == near) | (block_of(source) == second), factor * array, array)


def block_levels(rng, dims, cuts, least, largest):
    def one(position, shards_of):
        draws = jax.random.uniform(jax.random.fold_in(jax.random.fold_in(rng, 6), position), (shards_of,), jnp.float32, least / len(cuts), largest / len(cuts))
        return jnp.repeat(jnp.exp(draws), dims[position] // shards_of).reshape((-1,) + (1,) * (len(dims) - position - 1))

    loudness = one(*cuts[0])
    for cut in cuts[1:]:
        loudness = loudness * one(*cut)
    return loudness


def gaussian(key, shape, deviation, most, pieces=(), held_as=jnp.bfloat16):
    result = jax.random.normal(key, shape, jnp.float32) * deviation
    if len(pieces) > 0:
        result = block_levels(key, shape, pieces, -0.22, 0.18) * result
    return jnp.clip(result, min=-most, max=most).astype(held_as)


def heavy_noise(stream_key, dims, deviation, most, shards, heavy, held_as=jnp.bfloat16):
    drawn = deviation * jax.random.normal(stream_key, dims, jnp.float32)
    if shards:
        drawn = drawn * block_levels(stream_key, dims, shards, -0.22, 0.18)
    return jnp.clip(raised(drawn, jax.random.fold_in(stream_key, 3), *heavy), -most, most).astype(held_as)


def setup_inputs(seed: int = 0) -> dict:
    splits = jax.random.split(jax.random.key(seed), 7)
    return {
        "value_rows": gaussian(splits[0], (TOKENS, C), 1.0, 6.0, ((0, 128), (1, 4))),
        "gate_rows": gaussian(splits[1], (TOKENS, C), 1.0, 6.0, ((0, 128), (1, 4))),
        "conv_taps": gaussian(splits[2], (KW, C), KW ** -0.5, 1.0, ((1, 4),)),
        "norm_gain": jnp.clip(1.0 + 0.18 * jax.random.normal(splits[3], (C,), jnp.float32), 0.1, 1.9),
        "point_weight": gaussian(splits[4], (C, C), C ** -0.5, 0.1875, ((1, 4),)),
        "out_grad": heavy_noise(splits[5], (TOKENS, C), 1.0, 24.0, ((0, 128), (1, 4)), (0, 1, 128, 5.5)),
    }


EPS = 1e-06

def reference(value_rows, gate_rows, conv_taps, norm_gain, point_weight, out_grad):
    total_rows = value_rows.shape[0]
    block_rows = TOK_DEV
    block_count = total_rows // block_rows
    groups = C // GROUP
    gate_sig_all = jax.nn.sigmoid(gate_rows.astype(jnp.float32))
    gated_all = (value_rows.astype(jnp.float32) * gate_sig_all).astype(jnp.bfloat16)
    gated_pad = jnp.pad(gated_all, ((2 * HALF, 2 * HALF), (0, 0)))
    grad_pad = jnp.pad(out_grad, ((HALF, HALF), (0, 0)))
    taps_f = conv_taps.astype(jnp.float32)
    gain_g = norm_gain.astype(jnp.float32).reshape(groups, GROUP)
    extent = block_rows + 2 * HALF

    def one_block(carry, block_index):
        taps_acc, gain_acc, weight_acc = carry
        start = (block_index * block_rows).astype(jnp.int32)
        gated_wide = lax.dynamic_slice_in_dim(gated_pad, start, block_rows + 4 * HALF, 0)
        cotangent = lax.dynamic_slice_in_dim(grad_pad, start, extent, 0)
        value_f = lax.dynamic_slice_in_dim(value_rows, start, block_rows, 0).astype(jnp.float32)
        gate_sig = lax.dynamic_slice_in_dim(gate_sig_all, start, block_rows, 0)
        convolved = jnp.zeros((extent, C), jnp.float32)
        for tap_index in range(KW):
            convolved = convolved + taps_f[tap_index] * gated_wide[tap_index:tap_index + extent].astype(jnp.float32)
        grouped = convolved.reshape(extent, groups, GROUP)
        group_mean = lax.optimization_barrier(jnp.mean(grouped, axis=-1, keepdims=True))
        centred = grouped - group_mean
        inv_std = lax.rsqrt(lax.optimization_barrier(jnp.mean(centred * centred, axis=-1, keepdims=True)) + EPS)
        unit_conv = centred * inv_std
        pre_act = unit_conv * gain_g
        act_sig = jax.nn.sigmoid(pre_act)
        normed = (pre_act * act_sig).astype(jnp.bfloat16).reshape(extent, C)
        normed_grad = jnp.dot(cotangent, point_weight, preferred_element_type=jnp.float32).reshape(extent, groups, GROUP)
        own_grad = cotangent[HALF:HALF + block_rows]
        own_normed = normed[HALF:HALF + block_rows]
        weight_part = lax.dot_general(own_grad, own_normed, (((0,), (0,)), ((), ())), preferred_element_type=jnp.float32)
        act_grad = normed_grad * act_sig * (1.0 + pre_act * (1.0 - act_sig))
        gain_part = lax.optimization_barrier(jnp.sum((act_grad * unit_conv)[HALF:HALF + block_rows], axis=0)).reshape(C)
        hat_grad = act_grad * gain_g
        conv_grad = inv_std * (hat_grad - lax.optimization_barrier(jnp.mean(hat_grad, axis=-1, keepdims=True)) - unit_conv * lax.optimization_barrier(jnp.mean(hat_grad * unit_conv, axis=-1, keepdims=True)))
        conv_grad = conv_grad.reshape(extent, C)
        own_conv = conv_grad[HALF:HALF + block_rows]
        taps_part = jnp.stack([lax.optimization_barrier(jnp.sum(own_conv * gated_wide[HALF + tap_index:HALF + tap_index + block_rows].astype(jnp.float32), axis=0)) for tap_index in range(KW)])
        gated_grad = jnp.zeros((block_rows, C), jnp.float32)
        for tap_index in range(KW):
            lower = 2 * HALF - tap_index
            gated_grad = gated_grad + taps_f[tap_index] * conv_grad[lower:lower + block_rows]
        value_grad = (gated_grad * gate_sig).astype(jnp.bfloat16)
        gate_grad = (gated_grad * value_f * gate_sig * (1.0 - gate_sig)).astype(jnp.bfloat16)
        return ((taps_acc + taps_part, gain_acc + gain_part, weight_acc + weight_part), (value_grad, gate_grad))
    init = (jnp.zeros((KW, C), jnp.float32), jnp.zeros((C,), jnp.float32), jnp.zeros((C, C), jnp.float32))
    sums, blocks = lax.scan(one_block, init, jnp.arange(block_count, dtype=jnp.int32))
    taps_grad, gain_grad, weight_grad = sums
    value_grad = blocks[0].reshape(total_rows, C)
    gate_grad = blocks[1].reshape(total_rows, C)
    return (value_grad, gate_grad, taps_grad, gain_grad, weight_grad)
```

```python
import functools

import jax
import jax.numpy as jnp
from jax import lax
from jax.experimental import pallas as pl
from jax.experimental.pallas import tpu as pltpu
from jax.sharding import Mesh
from jax.sharding import PartitionSpec as P

GROUP = 64
SP = ("z", "x", "c")
EPS = 1e-06
ROWS = 1024
CH = 256
LANES = 128
PAD = 16
HALO = ROWS + 2 * PAD
KW = 31
F32 = jnp.float32
BF16 = jnp.bfloat16
CHUNK = 256
VMEM = pl.BlockSpec(memory_space=pltpu.VMEM)
SMEM = pl.BlockSpec(memory_space=pltpu.SMEM)


def group_mean(x, avg):
    high = x.astype(BF16)
    low = (x - high.astype(F32)).astype(BF16)
    return jnp.dot(high, avg, preferred_element_type=F32) + jnp.dot(
        low, avg, preferred_element_type=F32
    )


def averaging():
    rows = lax.broadcasted_iota(jnp.int32, (CH, CH), 0) // GROUP
    cols = lax.broadcasted_iota(jnp.int32, (CH, CH), 1) // GROUP
    return jnp.where(rows == cols, 1.0 / GROUP, 0.0).astype(BF16)


def convolve(src, taps_at, store):
    tiles = 4
    for block in range(CH // LANES):

        def some_rows(step, _, block=block):
            start = pl.multiple_of(step * (8 * tiles), 8 * tiles)
            sums = [None] * tiles
            for k in range(KW):
                tap = taps_at(k, block)
                for j in range(tiles):
                    part = src[block, pl.ds(start + 8 * j + k + 1, 8), :] * tap
                    sums[j] = part if sums[j] is None else sums[j] + part
            for j in range(tiles):
                store(block, pl.multiple_of(start + 8 * j, 8), sums[j])
            return 0

        lax.fori_loop(0, ROWS // (8 * tiles), some_rows, 0)


def forward_kernel(value, gate, before, after, taps, gain, wide, unit, inv, normed, conv):
    lanes = [slice(b * LANES, (b + 1) * LANES) for b in range(2)]
    for b in range(2):
        wide[b, 0:PAD, :] = before[:, lanes[b]].astype(F32)
        wide[b, PAD + ROWS : HALO, :] = after[:, lanes[b]].astype(F32)

    def gate_rows(step, _):
        start = pl.multiple_of(step * 64, 64)
        rows = pl.ds(start, 64)
        gated = (value[rows, :].astype(F32) * jax.nn.sigmoid(gate[rows, :].astype(F32))).astype(
            BF16
        )
        for b in range(2):
            wide[b, pl.ds(pl.multiple_of(start + PAD, 16), 64), :] = gated[:, lanes[b]].astype(F32)
        return 0

    lax.fori_loop(0, ROWS // 64, gate_rows, 0)

    def store(block, start, rows):
        conv[pl.ds(start, 8), lanes[block]] = rows

    convolve(
        wide, lambda k, b: jnp.broadcast_to(taps[k : k + 1, lanes[b]], (8, LANES)), store
    )
    avg = averaging()
    gain_row = gain[...]

    def norm_rows(step, _):
        rows = pl.ds(pl.multiple_of(step * CHUNK, CHUNK), CHUNK)
        raw = conv[rows, :]
        centred = raw - group_mean(raw, avg)
        scale = lax.rsqrt(group_mean(centred * centred, avg) + EPS)
        unit_rows = centred * scale
        pre = unit_rows * gain_row
        unit[rows, :] = unit_rows
        inv[rows, :] = scale
        normed[rows, :] = (pre * jax.nn.sigmoid(pre)).astype(BF16)
        return 0

    lax.fori_loop(0, ROWS // CHUNK, norm_rows, 0)


def early_kernel(me, own, left, right, weight, normed, partial, wgrad):
    y = me[0]
    blocks = ((own, lax.rem(y, 4)), (left, lax.rem(y + 3, 4)), (right, lax.rem(y + 1, 4)))
    weights = [weight[pl.ds(pl.multiple_of(at * CH, CH), CH), :] for _, at in blocks]

    def some_rows(step, _):
        rows = pl.ds(pl.multiple_of(step * CHUNK, CHUNK), CHUNK)
        total = None
        for (ref, _), w in zip(blocks, weights):
            part = jnp.dot(ref[rows, :], w, preferred_element_type=F32)
            total = part if total is None else total + part
        partial[rows, :] = total
        return 0

    lax.fori_loop(0, ROWS // CHUNK, some_rows, 0)
    for d, (ref, _) in enumerate(blocks):
        grads = lax.dot_general(
            ref[...], normed[...], (((0,), (0,)), ((), ())), preferred_element_type=F32
        )
        put_weight(wgrad, d, grads)


def put_weight(out, d, grads):
    pieces = grads.reshape(4, 8, 8, CH).astype(BF16)
    for near in range(4):
        for peer in range(8):
            out[peer, d * 4 + near] = pieces[near, peer]


def late_kernel(
    me, far, weight, normed, partial, unit, inv, gain, wide, grad, head, tail, sums, conv
):
    y = me[0]
    w = weight[pl.ds(pl.multiple_of(lax.rem(y + 2, 4) * CH, CH), CH), :]
    avg = averaging()
    gain_row = gain[...]

    def some_rows(step, gain_sum):
        start = pl.multiple_of(step * CHUNK, CHUNK)
        rows = pl.ds(start, CHUNK)
        normed_grad = partial[rows, :] + jnp.dot(far[rows, :], w, preferred_element_type=F32)
        u = unit[rows, :]
        pre = u * gain_row
        s = jax.nn.sigmoid(pre)
        act = normed_grad * s * (1.0 + pre * (1.0 - s))
        au = act * u
        hat = act * gain_row
        hat_unit = au * gain_row
        rows_grad = inv[rows, :] * (
            hat - group_mean(hat, avg) - u * group_mean(hat_unit, avg)
        )
        for b in range(2):
            conv[b, rows, :] = rows_grad[:, b * LANES : (b + 1) * LANES]
        return gain_sum + jnp.sum(au.reshape(CHUNK // 8, 8, CH), axis=0)

    gain_sum = lax.fori_loop(0, ROWS // CHUNK, some_rows, jnp.zeros((8, CH), F32))
    for b in range(2):
        cols = slice(b * LANES, (b + 1) * LANES)
        head[:, cols] = conv[b, 0:PAD, :]
        tail[:, cols] = conv[b, ROWS - PAD : ROWS, :]
        grad[b] = conv[b]

    put_weight(
        sums,
        0,
        lax.dot_general(
            far[...], normed[...], (((0,), (0,)), ((), ())), preferred_element_type=F32
        ),
    )

    halves = []
    for b in range(2):

        def tile(step, carry, b=b):
            start = pl.multiple_of(step * 8, 8)
            g = conv[b, pl.ds(start, 8), :]
            return tuple(
                acc + g * wide[b, pl.ds(start + k + 1, 8), :] for k, acc in enumerate(carry)
            )

        accs = lax.fori_loop(
            0, ROWS // 8, tile, tuple(jnp.zeros((8, LANES), F32) for _ in range(KW))
        )
        lines = [jnp.sum(a, axis=0, keepdims=True) for a in accs]
        halves.append(jnp.concatenate(lines, axis=0))
    taps = jnp.concatenate(
        [
            jnp.concatenate(halves, axis=1),
            jnp.sum(gain_sum, axis=0, keepdims=True),
        ],
        axis=0,
    ).astype(BF16)
    for peer in range(8):
        for part in range(2):
            line = (peer % 2) * 16 + part * 8
            sums[peer, 4 + part] = taps[line : line + 8]


def backward_kernel(value, gate, grad, before, after, taps, value_grad, gate_grad, wide, conv):
    lanes = [slice(b * LANES, (b + 1) * LANES) for b in range(2)]
    for b in range(2):
        wide[b, 0:PAD, :] = before[:, lanes[b]]
        wide[b, PAD : PAD + ROWS, :] = grad[b]
        wide[b, PAD + ROWS : HALO, :] = after[:, lanes[b]]

    def store(block, start, rows):
        conv[pl.ds(start, 8), lanes[block]] = rows

    convolve(
        wide,
        lambda k, b: jnp.broadcast_to(taps[KW - 1 - k : KW - k, lanes[b]], (8, LANES)),
        store,
    )

    def finish(step, _):
        rows = pl.ds(pl.multiple_of(step * 64, 64), 64)
        s = jax.nn.sigmoid(gate[rows, :].astype(F32))
        down = conv[rows, :] * s
        value_grad[rows, :] = down.astype(BF16)
        gate_grad[rows, :] = (down * value[rows, :].astype(F32) * (1.0 - s)).astype(BF16)
        return 0

    lax.fori_loop(0, ROWS // 64, finish, 0)


def middle_kernel(me, early, late, out):
    y = me[0]
    taps = late[0, 4:6].astype(F32)
    for peer in range(1, 8):
        taps = taps + late[peer, 4:6].astype(F32)
    taps = taps.astype(BF16)
    for d, at in enumerate((y, y + 3, y + 1, y + 2)):
        home = lax.rem(at, 4)
        src, base = (early, d * 4) if d < 3 else (late, 0)
        for near in range(4):
            total = src[0, base + near].astype(F32)
            for peer in range(1, 8):
                total = total + src[peer, base + near].astype(F32)
            out[home * 4 + near, 0] = total.astype(BF16)
            out[home * 4 + near, 1:3] = taps


def call(kernel, outs, specs, scratch=(), name=None, cost=None):
    return pl.pallas_call(
        kernel,
        out_shape=outs,
        in_specs=specs,
        out_specs=jax.tree.map(lambda _: VMEM, outs),
        scratch_shapes=scratch,
        name=name,
        cost_estimate=cost,
        compiler_params=pltpu.CompilerParams(vmem_limit_bytes=48 * 1024 * 1024),
    )


def shape(*dims, dtype=F32):
    return jax.ShapeDtypeStruct(dims, dtype)


def cost(us):
    return pl.CostEstimate(flops=int(us * 1e-6 * 2e14), bytes_accessed=2**20, transcendentals=0)


def ring(size, by):
    return [(i, (i + by) % size) for i in range(size)]


def per_device(value_rows, gate_rows, conv_taps, norm_gain, point_weight, out_grad):
    peers = lax.axis_size(SP)
    up = [(i, i + 1) for i in range(peers - 1)]
    down = [(j, i) for i, j in up]
    me = lax.axis_index("tp").astype(jnp.int32).reshape(1)
    taps = conv_taps.astype(F32)
    gain = norm_gain.reshape(1, CH)

    left = lax.ppermute(out_grad, "tp", ring(4, 1))
    right = lax.ppermute(out_grad, "tp", ring(4, 3))
    far = lax.ppermute(out_grad, "tp", ring(4, 2))

    def gated_of(rows):
        return (
            value_rows[rows].astype(F32) * jax.nn.sigmoid(gate_rows[rows].astype(F32))
        ).astype(BF16)

    before = lax.ppermute(gated_of(slice(ROWS - PAD, ROWS)), SP, up)
    after = lax.ppermute(gated_of(slice(0, PAD)), SP, down)

    wide, unit, inv, normed = call(
        forward_kernel,
        (shape(2, HALO, LANES), shape(ROWS, CH), shape(ROWS, CH), shape(ROWS, CH, dtype=BF16)),
        [VMEM] * 6,
        [pltpu.VMEM((ROWS, CH), F32)],
        "forward",
        cost(7),
    )(value_rows, gate_rows, before, after, taps, gain)

    partial, wgrad = call(
        early_kernel,
        (shape(ROWS, CH), shape(8, 12, 8, CH, dtype=BF16)),
        [SMEM] + [VMEM] * 5,
        (),
        "early",
        cost(4),
    )(me, out_grad, left, right, point_weight, normed)
    early = lax.all_to_all(wgrad, ("x", "c"), 0, 0, tiled=True)

    grad, head, tail, sums = call(
        late_kernel,
        (
            shape(2, ROWS, LANES),
            shape(PAD, CH),
            shape(PAD, CH),
            shape(8, 6, 8, CH, dtype=BF16),
        ),
        [SMEM] + [VMEM] * 8,
        [pltpu.VMEM((2, ROWS, LANES), F32)],
        "late",
        cost(8),
    )(me, far, point_weight, normed, partial, unit, inv, gain, wide)
    late = lax.all_to_all(sums, ("x", "c"), 0, 0, tiled=True)

    grad_before = lax.ppermute(tail, SP, up)
    grad_after = lax.ppermute(head, SP, down)
    value_grad, gate_grad = call(
        backward_kernel,
        (shape(ROWS, CH, dtype=BF16), shape(ROWS, CH, dtype=BF16)),
        [VMEM] * 6,
        [pltpu.VMEM((2, HALO, LANES), F32), pltpu.VMEM((ROWS, CH), F32)],
        "backward",
        cost(6),
    )(value_rows, gate_rows, grad, grad_before, grad_after, taps)

    sent = call(
        middle_kernel,
        shape(16, 3, 8, CH, dtype=BF16),
        [SMEM, VMEM, VMEM],
        (),
        "middle",
        cost(1),
    )(me, early, late)
    whole = jnp.sum(lax.all_to_all(sent, "z", 0, 0, tiled=True).astype(F32), axis=0)
    mine = whole[1:3].reshape(16, CH)
    other = lax.ppermute(mine, "c", ring(2, 1))
    first = lax.axis_index("c") == 0
    low = jnp.where(first, mine, other)
    high = jnp.where(first, other, mine)
    return value_grad, gate_grad, jnp.concatenate([low, high[:15]]), high[15], whole[0]


def solution(mesh):
    finer = Mesh(mesh.devices.reshape(16, 4, 2, mesh.shape["tp"]), ("z", "x", "c", "tp"))
    return jax.shard_map(
        per_device,
        mesh=finer,
        in_specs=(P(SP, "tp"), P(SP, "tp"), P(None, "tp"), P("tp"), P(None, "tp"), P(SP, "tp")),
        out_specs=(P(SP, "tp"), P(SP, "tp"), P(None, "tp"), P("tp"), P(SP, "tp")),
        check_vma=False,
    )
```

```python
import jax
import jax.numpy as jnp
from jax import lax
from jax.experimental import pallas as pl
from jax.experimental.pallas import tpu as pltpu
from jax.sharding import Mesh
from jax.sharding import PartitionSpec as P


GROUP = 64
SP = ("z", "x", "c")
EPS = 1e-06
ROWS = 1024
CH = 256
LANES = 128
PAD = 16
HALO = ROWS + 2 * PAD
KW = 31
F32 = jnp.float32
BF16 = jnp.bfloat16
CHUNK = 256
VMEM = pl.BlockSpec(memory_space=pltpu.VMEM)
SMEM = pl.BlockSpec(memory_space=pltpu.SMEM)


def group_mean(x, avg):
    high = x.astype(BF16)
    low = (x - high.astype(F32)).astype(BF16)
    return jnp.dot(high, avg, preferred_element_type=F32) + jnp.dot(
        low, avg, preferred_element_type=F32
    )


def averaging():
    rows = lax.broadcasted_iota(jnp.int32, (CH, CH), 0) // GROUP
    cols = lax.broadcasted_iota(jnp.int32, (CH, CH), 1) // GROUP
    return jnp.where(rows == cols, 1.0 / GROUP, 0.0).astype(BF16)


def convolve(src, taps_at, store):
    tiles = 4
    for block in range(CH // LANES):

        def some_rows(step, _, block=block):
            start = pl.multiple_of(step * (8 * tiles), 8 * tiles)
            sums = [None] * tiles
            for k in range(KW):
                tap = taps_at(k, block)
                for j in range(tiles):
                    part = src[block, pl.ds(start + 8 * j + k + 1, 8), :] * tap
                    sums[j] = part if sums[j] is None else sums[j] + part
            for j in range(tiles):
                store(block, pl.multiple_of(start + 8 * j, 8), sums[j])
            return 0

        lax.fori_loop(0, ROWS // (8 * tiles), some_rows, 0)


def sides(second, inner, outer):
    return jnp.where(second, inner, outer), jnp.where(second, outer, inner)


def forward_kernel(
    me, value, gate, inner, outer, taps, gain, wide, unit, inv, slope, normed, conv
):
    lanes = [slice(b * LANES, (b + 1) * LANES) for b in range(2)]
    before, after = sides(me[1] == 1, inner[...].astype(F32), outer[...].astype(F32))
    for b in range(2):
        wide[b, 0:PAD, :] = before[:, lanes[b]]
        wide[b, PAD + ROWS : HALO, :] = after[:, lanes[b]]

    def gate_rows(step, _):
        start = pl.multiple_of(step * 64, 64)
        rows = pl.ds(start, 64)
        gated = (value[rows, :].astype(F32) * jax.nn.sigmoid(gate[rows, :].astype(F32))).astype(
            BF16
        )
        for b in range(2):
            wide[b, pl.ds(pl.multiple_of(start + PAD, 16), 64), :] = gated[:, lanes[b]].astype(F32)
        return 0

    lax.fori_loop(0, ROWS // 64, gate_rows, 0)

    def store(block, start, rows):
        conv[pl.ds(start, 8), lanes[block]] = rows

    lines = taps[...].astype(F32)
    convolve(
        wide, lambda k, b: jnp.broadcast_to(lines[k : k + 1, lanes[b]], (8, LANES)), store
    )
    avg = averaging()
    gain_row = gain[...]

    def norm_rows(step, _):
        rows = pl.ds(pl.multiple_of(step * CHUNK, CHUNK), CHUNK)
        raw = conv[rows, :]
        centred = raw - group_mean(raw, avg)
        scale = lax.rsqrt(group_mean(centred * centred, avg) + EPS)
        unit_rows = centred * scale
        pre = unit_rows * gain_row
        s = jax.nn.sigmoid(pre)
        unit[rows, :] = unit_rows
        inv[rows, :] = scale
        slope[rows, :] = s * (1.0 + pre * (1.0 - s))
        normed[rows, :] = (pre * s).astype(BF16)
        return 0

    lax.fori_loop(0, ROWS // CHUNK, norm_rows, 0)


def early_kernel(me, own, left, right, weight, normed, partial, wgrad):
    y = me[0]
    blocks = ((own, lax.rem(y, 4)), (left, lax.rem(y + 3, 4)), (right, lax.rem(y + 1, 4)))
    weights = [weight[pl.ds(pl.multiple_of(at * CH, CH), CH), :] for _, at in blocks]

    def some_rows(step, _):
        rows = pl.ds(pl.multiple_of(step * CHUNK, CHUNK), CHUNK)
        total = None
        for (ref, _), w in zip(blocks, weights):
            part = jnp.dot(ref[rows, :], w, preferred_element_type=F32)
            total = part if total is None else total + part
        partial[rows, :] = total
        return 0

    lax.fori_loop(0, ROWS // CHUNK, some_rows, 0)
    for d, (ref, _) in enumerate(blocks):
        grads = lax.dot_general(
            ref[...], normed[...], (((0,), (0,)), ((), ())), preferred_element_type=F32
        )
        put_weight(wgrad, d, grads)


def put_weight(out, d, grads):
    pieces = grads.reshape(4, 8, 8, CH).astype(BF16)
    for near in range(4):
        for peer in range(8):
            out[peer, d * 4 + near] = pieces[near, peer]


def late_kernel(
    me, far, weight, normed, partial, unit, inv, slope, gain, wide, begun, grad, swap_in, swap_out, sums
):
    y = me[0]
    w = weight[pl.ds(pl.multiple_of(lax.rem(y + 2, 4) * CH, CH), CH), :]
    avg = averaging()
    gain_row = gain[...]

    def some_rows(step, gain_sum):
        start = pl.multiple_of(step * CHUNK, CHUNK)
        rows = pl.ds(start, CHUNK)
        normed_grad = partial[rows, :] + jnp.dot(far[rows, :], w, preferred_element_type=F32)
        u = unit[rows, :]
        act = normed_grad * slope[rows, :]
        au = act * u
        hat = act * gain_row
        hat_unit = au * gain_row
        rows_grad = inv[rows, :] * (
            hat - group_mean(hat, avg) - u * group_mean(hat_unit, avg)
        )
        for b in range(2):
            grad[b, rows, :] = rows_grad[:, b * LANES : (b + 1) * LANES]
        return gain_sum + jnp.sum(au.reshape(CHUNK // 8, 8, CH), axis=0)

    gain_sum = lax.fori_loop(0, ROWS // CHUNK, some_rows, jnp.zeros((8, CH), F32))
    for b in range(2):
        cols = slice(b * LANES, (b + 1) * LANES)
        head, tail = grad[b, 0:PAD, :], grad[b, ROWS - PAD : ROWS, :]
        swap_in[:, cols], swap_out[:, cols] = sides(me[1] == 1, head, tail)

    put_weight(
        sums,
        3,
        lax.dot_general(
            far[...], normed[...], (((0,), (0,)), ((), ())), preferred_element_type=F32
        ),
    )

    halves = []
    for b in range(2):

        def tile(step, carry, b=b):
            start = pl.multiple_of(step * 8, 8)
            g = grad[b, pl.ds(start, 8), :]
            return tuple(
                acc + g * wide[b, pl.ds(start + k + 1, 8), :] for k, acc in enumerate(carry)
            )

        accs = lax.fori_loop(
            0, ROWS // 8, tile, tuple(jnp.zeros((8, LANES), F32) for _ in range(KW))
        )
        lines = [jnp.sum(a, axis=0, keepdims=True) for a in accs]
        halves.append(jnp.concatenate(lines, axis=0))
    taps = jnp.concatenate(
        [
            jnp.concatenate(halves, axis=1),
            jnp.sum(gain_sum, axis=0, keepdims=True),
        ],
        axis=0,
    ).astype(BF16)
    for peer in range(8):
        for part in range(2):
            line = (peer % 2) * 16 + part * 8
            sums[peer, 16 + part] = taps[line : line + 8]


def backward_kernel(
    me, value, gate, grad, inner, outer, taps, value_grad, gate_grad, wide, conv
):
    before, after = sides(me[1] == 1, inner[...], outer[...])
    lines = taps[...].astype(F32)
    lanes = [slice(b * LANES, (b + 1) * LANES) for b in range(2)]
    for b in range(2):
        wide[b, 0:PAD, :] = before[:, lanes[b]]
        wide[b, PAD : PAD + ROWS, :] = grad[b]
        wide[b, PAD + ROWS : HALO, :] = after[:, lanes[b]]

    def store(block, start, rows):
        conv[pl.ds(start, 8), lanes[block]] = rows

    convolve(
        wide,
        lambda k, b: jnp.broadcast_to(lines[KW - 1 - k : KW - k, lanes[b]], (8, LANES)),
        store,
    )

    def finish(step, _):
        rows = pl.ds(pl.multiple_of(step * 64, 64), 64)
        s = jax.nn.sigmoid(gate[rows, :].astype(F32))
        down = conv[rows, :] * s
        value_grad[rows, :] = down.astype(BF16)
        gate_grad[rows, :] = (down * value[rows, :].astype(F32) * (1.0 - s)).astype(BF16)
        return 0

    lax.fori_loop(0, ROWS // 64, finish, 0)


def middle_kernel(me, late, out):
    y = me[0]
    taps = late[0, 16:18].astype(F32)
    for peer in range(1, 8):
        taps = taps + late[peer, 16:18].astype(F32)
    taps = taps.astype(BF16)
    for d, at in enumerate((y, y + 3, y + 1, y + 2)):
        home = lax.rem(at, 4)
        for near in range(4):
            total = late[0, d * 4 + near].astype(F32)
            for peer in range(1, 8):
                total = total + late[peer, d * 4 + near].astype(F32)
            out[home * 4 + near, 0] = total.astype(BF16)
            out[home * 4 + near, 1:3] = taps


def whole_kernel(got, weight, mine):
    total = got[0].astype(F32)
    for peer in range(1, 16):
        total = total + got[peer].astype(F32)
    weight[...] = total[0]
    mine[0:8] = total[1]
    mine[8:16] = total[2]


def last_kernel(me, mine, other, taps, gain):
    low, high = sides(me[1] == 1, other[...], mine[...])
    taps[0:16] = low
    taps[16:31] = high[:15]
    gain[...] = high[15:16]


def call(kernel, outs, specs, scratch=(), cost=None, alias={}):
    return pl.pallas_call(
        kernel,
        out_shape=outs,
        in_specs=specs,
        out_specs=jax.tree.map(lambda _: VMEM, outs),
        scratch_shapes=scratch,
        cost_estimate=cost,
        input_output_aliases=alias,
        compiler_params=pltpu.CompilerParams(vmem_limit_bytes=8 * 1024 * 1024),
    )


def shape(*dims, dtype=F32):
    return jax.ShapeDtypeStruct(dims, dtype)


def cost(us):
    return pl.CostEstimate(flops=int(us * 1e-6 * 2e14), bytes_accessed=2**20, transcendentals=0)


def ring(size, by):
    return [(i, (i + by) % size) for i in range(size)]


def body(value_rows, gate_rows, conv_taps, norm_gain, point_weight, out_grad):
    peers = lax.axis_size(SP)
    pairs = [(i, i ^ 1) for i in range(peers)]
    apart = [(i, i + 1) for i in range(1, peers - 1, 2)]
    apart = apart + [(j, i) for i, j in apart]
    second = lax.axis_index("c").astype(jnp.int32)
    me = jnp.stack([lax.axis_index("tp").astype(jnp.int32), second])
    gain = norm_gain.reshape(1, CH)

    def exchange(array, axis):
        return lax.all_to_all(array, axis, 0, 0, tiled=True)

    def gated_of(rows):
        return (
            value_rows[rows].astype(F32) * jax.nn.sigmoid(gate_rows[rows].astype(F32))
        ).astype(BF16)

    swap_in, swap_out = sides(
        second == 1, gated_of(slice(0, PAD)), gated_of(slice(ROWS - PAD, ROWS))
    )
    left = lax.ppermute(out_grad, "tp", ring(4, 1))
    right = lax.ppermute(out_grad, "tp", ring(4, 3))
    inner = lax.ppermute(swap_in, SP, pairs)
    outer = lax.ppermute(swap_out, SP, apart)
    far = lax.ppermute(out_grad, "tp", ring(4, 2))

    wide, unit, inv, slope, normed = call(
        forward_kernel,
        (
            shape(2, HALO, LANES),
            shape(ROWS, CH),
            shape(ROWS, CH),
            shape(ROWS, CH),
            shape(ROWS, CH, dtype=BF16),
        ),
        [SMEM] + [VMEM] * 6,
        [pltpu.VMEM((ROWS, CH), F32)],
        cost(7),
    )(me, value_rows, gate_rows, inner, outer, conv_taps, gain)

    partial, wgrad = call(
        early_kernel,
        (shape(ROWS, CH), shape(8, 18, 8, CH, dtype=BF16)),
        [SMEM] + [VMEM] * 5,
        (),
        cost(4),
    )(me, out_grad, left, right, point_weight, normed)

    grad, swap_in, swap_out, sums = call(
        late_kernel,
        (
            shape(2, ROWS, LANES),
            shape(PAD, CH),
            shape(PAD, CH),
            shape(8, 18, 8, CH, dtype=BF16),
        ),
        [SMEM] + [VMEM] * 10,
        (),
        cost(8),
        {10: 3},
    )(me, far, point_weight, normed, partial, unit, inv, slope, gain, wide, wgrad)
    late = exchange(sums, ("x", "c"))

    sent = call(middle_kernel, shape(16, 3, 8, CH, dtype=BF16), [SMEM, VMEM], (), cost(1))(me, late)
    got = exchange(sent, "z")

    inner = lax.ppermute(swap_in, SP, pairs)
    outer = lax.ppermute(swap_out, SP, apart)
    value_grad, gate_grad = call(
        backward_kernel,
        (shape(ROWS, CH, dtype=BF16), shape(ROWS, CH, dtype=BF16)),
        [SMEM] + [VMEM] * 6,
        [pltpu.VMEM((2, HALO, LANES), F32), pltpu.VMEM((ROWS, CH), F32)],
        cost(6),
    )(me, value_rows, gate_rows, grad, inner, outer, conv_taps)

    got, value_grad, gate_grad = lax.optimization_barrier((got, value_grad, gate_grad))
    weight_grad, mine = call(whole_kernel, (shape(8, CH), shape(16, CH)), [VMEM], (), cost(1))(got)
    other = lax.ppermute(mine, "c", ring(2, 1))
    taps_grad, gain_grad = call(
        last_kernel, (shape(KW, CH), shape(1, CH)), [SMEM, VMEM, VMEM], (), cost(1)
    )(me, mine, other)
    return value_grad, gate_grad, taps_grad, gain_grad.reshape(CH), weight_grad


def solution(mesh):
    finer = Mesh(mesh.devices.reshape(16, 4, 2, mesh.shape["tp"]), ("z", "x", "c", "tp"))
    return jax.shard_map(
        body,
        mesh=finer,
        in_specs=(P(SP, "tp"), P(SP, "tp"), P(None, "tp"), P("tp"), P(None, "tp"), P(SP, "tp")),
        out_specs=(P(SP, "tp"), P(SP, "tp"), P(None, "tp"), P("tp"), P(SP, "tp")),
        check_vma=False,
    )
```

```python
import jax
import jax.numpy as jnp
from jax import lax
from jax.experimental import pallas as pl
from jax.experimental.pallas import tpu as pltpu
from jax.sharding import Mesh
from jax.sharding import PartitionSpec as P


GROUP = 64
SP = ("z", "x", "c")
EPS = 1e-06
ROWS = 1024
CH = 256
LANES = 128
PAD = 16
HALO = ROWS + 2 * PAD
KW = 31
F32 = jnp.float32
BF16 = jnp.bfloat16
CHUNK = 256
VMEM = pl.BlockSpec(memory_space=pltpu.VMEM)


def group_mean(x, avg):
    high = x.astype(BF16)
    low = (x - high.astype(F32)).astype(BF16)
    return jnp.dot(high, avg, preferred_element_type=F32) + jnp.dot(
        low, avg, preferred_element_type=F32
    )


def averaging():
    rows = lax.broadcasted_iota(jnp.int32, (CH, CH), 0) // GROUP
    cols = lax.broadcasted_iota(jnp.int32, (CH, CH), 1) // GROUP
    return jnp.where(rows == cols, 1.0 / GROUP, 0.0).astype(BF16)


def convolve(src, taps_at, store):
    tiles = 4
    for block in range(CH // LANES):

        def some_rows(step, _, block=block):
            start = pl.multiple_of(step * (8 * tiles), 8 * tiles)
            sums = [None] * tiles
            for k in range(KW):
                tap = taps_at(k, block)
                for j in range(tiles):
                    part = src[block, pl.ds(start + 8 * j + k + 1, 8), :] * tap
                    sums[j] = part if sums[j] is None else sums[j] + part
            for j in range(tiles):
                store(block, pl.multiple_of(start + 8 * j, 8), sums[j])
            return 0

        lax.fori_loop(0, ROWS // (8 * tiles), some_rows, 0)


def is_second():
    return lax.axis_index("c") == 1


def sides(second, inner, outer):
    return jnp.where(second, inner, outer), jnp.where(second, outer, inner)


def edge_kernel(value_head, gate_head, value_tail, gate_tail, swap_in, swap_out):
    def gated(value, gate):
        return value[...].astype(F32) * jax.nn.sigmoid(gate[...].astype(F32))

    inner, outer = sides(is_second(), gated(value_head, gate_head), gated(value_tail, gate_tail))
    swap_in[...] = inner.astype(BF16)
    swap_out[...] = outer.astype(BF16)


def forward_kernel(
    value, gate, inner, outer, taps, gain, wide, unit, inv, slope, normed, conv
):
    lanes = [slice(b * LANES, (b + 1) * LANES) for b in range(2)]
    before, after = sides(is_second(), inner[...].astype(F32), outer[...].astype(F32))
    for b in range(2):
        wide[b, 0:PAD, :] = before[:, lanes[b]]
        wide[b, PAD + ROWS : HALO, :] = after[:, lanes[b]]

    def gate_rows(step, _):
        start = pl.multiple_of(step * 64, 64)
        rows = pl.ds(start, 64)
        gated = (value[rows, :].astype(F32) * jax.nn.sigmoid(gate[rows, :].astype(F32))).astype(
            BF16
        )
        for b in range(2):
            wide[b, pl.ds(pl.multiple_of(start + PAD, 16), 64), :] = gated[:, lanes[b]].astype(F32)
        return 0

    lax.fori_loop(0, ROWS // 64, gate_rows, 0)

    def store(block, start, rows):
        conv[pl.ds(start, 8), lanes[block]] = rows

    lines = taps[...].astype(F32)
    convolve(
        wide, lambda k, b: jnp.broadcast_to(lines[k : k + 1, lanes[b]], (8, LANES)), store
    )
    avg = averaging()
    gain_row = gain[...]

    def norm_rows(step, _):
        rows = pl.ds(pl.multiple_of(step * CHUNK, CHUNK), CHUNK)
        raw = conv[rows, :]
        centred = raw - group_mean(raw, avg)
        scale = lax.rsqrt(group_mean(centred * centred, avg) + EPS)
        unit_rows = centred * scale
        pre = unit_rows * gain_row
        s = jax.nn.sigmoid(pre)
        unit[rows, :] = unit_rows
        inv[rows, :] = scale
        slope[rows, :] = s * (1.0 + pre * (1.0 - s))
        normed[rows, :] = (pre * s).astype(BF16)
        return 0

    lax.fori_loop(0, ROWS // CHUNK, norm_rows, 0)


def early_kernel(own, left, right, weight, normed, partial, wgrad):
    y = lax.axis_index("tp")
    blocks = ((own, lax.rem(y, 4)), (left, lax.rem(y + 3, 4)), (right, lax.rem(y + 1, 4)))
    weights = [weight[pl.ds(pl.multiple_of(at * CH, CH), CH), :] for _, at in blocks]

    def some_rows(step, _):
        rows = pl.ds(pl.multiple_of(step * CHUNK, CHUNK), CHUNK)
        total = None
        for (ref, _), w in zip(blocks, weights):
            part = jnp.dot(ref[rows, :], w, preferred_element_type=F32)
            total = part if total is None else total + part
        partial[rows, :] = total
        return 0

    lax.fori_loop(0, ROWS // CHUNK, some_rows, 0)
    for d, (ref, _) in enumerate(blocks):
        grads = lax.dot_general(
            ref[...], normed[...], (((0,), (0,)), ((), ())), preferred_element_type=F32
        )
        put_weight(wgrad, d, grads)


def put_weight(out, d, grads):
    pieces = grads.reshape(4, 8, 8, CH).astype(BF16)
    for near in range(4):
        for peer in range(8):
            out[peer, d * 4 + near] = pieces[near, peer]


def late_kernel(
    far, weight, normed, partial, unit, inv, slope, gain, wide, begun, grad, swap_in, swap_out, sums
):
    y = lax.axis_index("tp")
    w = weight[pl.ds(pl.multiple_of(lax.rem(y + 2, 4) * CH, CH), CH), :]
    avg = averaging()
    gain_row = gain[...]

    def some_rows(step, gain_sum):
        start = pl.multiple_of(step * CHUNK, CHUNK)
        rows = pl.ds(start, CHUNK)
        normed_grad = partial[rows, :] + jnp.dot(far[rows, :], w, preferred_element_type=F32)
        u = unit[rows, :]
        act = normed_grad * slope[rows, :]
        au = act * u
        hat = act * gain_row
        hat_unit = au * gain_row
        rows_grad = inv[rows, :] * (
            hat - group_mean(hat, avg) - u * group_mean(hat_unit, avg)
        )
        for b in range(2):
            grad[b, rows, :] = rows_grad[:, b * LANES : (b + 1) * LANES]
        return gain_sum + jnp.sum(au.reshape(CHUNK // 8, 8, CH), axis=0)

    gain_sum = lax.fori_loop(0, ROWS // CHUNK, some_rows, jnp.zeros((8, CH), F32))
    for b in range(2):
        cols = slice(b * LANES, (b + 1) * LANES)
        head, tail = grad[b, 0:PAD, :], grad[b, ROWS - PAD : ROWS, :]
        swap_in[:, cols], swap_out[:, cols] = sides(is_second(), head, tail)

    for peer in range(8):
        sums[peer, 0:12] = begun[peer]
    put_weight(
        sums,
        3,
        lax.dot_general(
            far[...], normed[...], (((0,), (0,)), ((), ())), preferred_element_type=F32
        ),
    )

    halves = []
    for b in range(2):
        lines = []
        for group in (range(0, 16), range(16, KW)):

            def tiles(step, carry, b=b, group=group):
                accs = list(carry)
                for j in range(4):
                    start = pl.multiple_of(step * 32, 32) + 8 * j
                    g = grad[b, pl.ds(start, 8), :]
                    for i, k in enumerate(group):
                        accs[i] = accs[i] + g * wide[b, pl.ds(start + k + 1, 8), :]
                return tuple(accs)

            accs = lax.fori_loop(
                0, ROWS // 32, tiles, tuple(jnp.zeros((8, LANES), F32) for _ in group)
            )
            lines += [jnp.sum(a, axis=0, keepdims=True) for a in accs]
        halves.append(jnp.concatenate(lines, axis=0))
    taps = jnp.concatenate(
        [
            jnp.concatenate(halves, axis=1),
            jnp.sum(gain_sum, axis=0, keepdims=True),
        ],
        axis=0,
    ).astype(BF16)
    for peer in range(8):
        for part in range(2):
            line = (peer % 2) * 16 + part * 8
            sums[peer, 16 + part] = taps[line : line + 8]


def backward_kernel(
    value, gate, grad, inner, outer, taps, value_grad, gate_grad, wide, conv
):
    before, after = sides(is_second(), inner[...], outer[...])
    lines = taps[...].astype(F32)
    lanes = [slice(b * LANES, (b + 1) * LANES) for b in range(2)]
    for b in range(2):
        wide[b, 0:PAD, :] = before[:, lanes[b]]
        wide[b, PAD : PAD + ROWS, :] = grad[b]
        wide[b, PAD + ROWS : HALO, :] = after[:, lanes[b]]

    def store(block, start, rows):
        conv[pl.ds(start, 8), lanes[block]] = rows

    convolve(
        wide,
        lambda k, b: jnp.broadcast_to(lines[KW - 1 - k : KW - k, lanes[b]], (8, LANES)),
        store,
    )

    def finish(step, _):
        rows = pl.ds(pl.multiple_of(step * 64, 64), 64)
        s = jax.nn.sigmoid(gate[rows, :].astype(F32))
        down = conv[rows, :] * s
        value_grad[rows, :] = down.astype(BF16)
        gate_grad[rows, :] = (down * value[rows, :].astype(F32) * (1.0 - s)).astype(BF16)
        return 0

    lax.fori_loop(0, ROWS // 64, finish, 0)


def middle_kernel(late, out):
    y = lax.axis_index("tp")
    taps = late[0, 16:18].astype(F32)
    for peer in range(1, 8):
        taps = taps + late[peer, 16:18].astype(F32)
    taps = taps.astype(BF16)
    for d, at in enumerate((y, y + 3, y + 1, y + 2)):
        home = lax.rem(at, 4)
        for near in range(4):
            total = late[0, d * 4 + near].astype(F32)
            for peer in range(1, 8):
                total = total + late[peer, d * 4 + near].astype(F32)
            out[home * 4 + near, 0] = total.astype(BF16)
            out[home * 4 + near, 1:3] = taps


def whole_kernel(got, weight, mine):
    total = got[0].astype(F32)
    for peer in range(1, 16):
        total = total + got[peer].astype(F32)
    weight[...] = total[0]
    mine[0:8] = total[1]
    mine[8:16] = total[2]


def last_kernel(mine, other, taps, gain):
    low, high = sides(is_second(), other[...], mine[...])
    taps[0:16] = low
    taps[16:31] = high[:15]
    gain[...] = high[15:16]


def call(kernel, outs, specs, scratch=(), cost=None):
    return pl.pallas_call(
        kernel,
        out_shape=outs,
        in_specs=specs,
        out_specs=jax.tree.map(lambda _: VMEM, outs),
        scratch_shapes=scratch,
        cost_estimate=cost,
        compiler_params=pltpu.CompilerParams(vmem_limit_bytes=8 * 1024 * 1024),
    )


def shape(*dims, dtype=F32):
    return jax.ShapeDtypeStruct(dims, dtype)


def cost(us):
    return pl.CostEstimate(flops=int(us * 1e-6 * 2e14), bytes_accessed=2**20, transcendentals=0)


def ring(size, by):
    return [(i, (i + by) % size) for i in range(size)]


def body(value_rows, gate_rows, conv_taps, norm_gain, point_weight, out_grad):
    peers = lax.axis_size(SP)
    pairs = [(i, i ^ 1) for i in range(peers)]
    apart = [(i, i + 1) for i in range(1, peers - 1, 2)]
    apart = apart + [(j, i) for i, j in apart]
    gain = norm_gain.reshape(1, CH)

    def exchange(array, axis):
        return lax.all_to_all(array, axis, 0, 0, tiled=True)

    first_rows = pl.BlockSpec((PAD, CH), lambda i: (0, 0))
    last_rows = pl.BlockSpec((PAD, CH), lambda i: (ROWS // PAD - 1, 0))
    swap_in, swap_out = pl.pallas_call(
        edge_kernel,
        out_shape=(shape(PAD, CH, dtype=BF16),) * 2,
        grid=(1,),
        in_specs=[first_rows, first_rows, last_rows, last_rows],
        out_specs=(first_rows, first_rows),
        name="edges",
    )(value_rows, gate_rows, value_rows, gate_rows)
    left = lax.ppermute(out_grad, "tp", ring(4, 1))
    right = lax.ppermute(out_grad, "tp", ring(4, 3))
    far = lax.ppermute(out_grad, "tp", ring(4, 2))
    inner = lax.ppermute(swap_in, SP, pairs)
    outer = lax.ppermute(swap_out, SP, apart)

    wide, unit, inv, slope, normed = call(
        forward_kernel,
        (
            shape(2, HALO, LANES),
            shape(ROWS, CH),
            shape(ROWS, CH),
            shape(ROWS, CH),
            shape(ROWS, CH, dtype=BF16),
        ),
        [VMEM] * 6,
        [pltpu.VMEM((ROWS, CH), F32)],
        cost(7),
    )(value_rows, gate_rows, inner, outer, conv_taps, gain)

    partial, wgrad = call(
        early_kernel, (shape(ROWS, CH), shape(8, 12, 8, CH, dtype=BF16)), [VMEM] * 5, (), cost(4)
    )(out_grad, left, right, point_weight, normed)

    grad, swap_in, swap_out, sums = call(
        late_kernel,
        (
            shape(2, ROWS, LANES),
            shape(PAD, CH),
            shape(PAD, CH),
            shape(8, 18, 8, CH, dtype=BF16),
        ),
        [VMEM] * 10,
        (),
        cost(8),
    )(far, point_weight, normed, partial, unit, inv, slope, gain, wide, wgrad)
    late = exchange(sums, ("x", "c"))

    inner = lax.ppermute(swap_in, SP, pairs)
    outer = lax.ppermute(swap_out, SP, apart)
    late, inner, outer = lax.optimization_barrier((late, inner, outer))
    sent = call(middle_kernel, shape(16, 3, 8, CH, dtype=BF16), [VMEM], (), cost(1))(late)
    got = exchange(sent, "z")

    value_grad, gate_grad = call(
        backward_kernel,
        (shape(ROWS, CH, dtype=BF16), shape(ROWS, CH, dtype=BF16)),
        [VMEM] * 6,
        [pltpu.VMEM((2, HALO, LANES), F32), pltpu.VMEM((ROWS, CH), F32)],
        cost(6),
    )(value_rows, gate_rows, grad, inner, outer, conv_taps)

    got, value_grad, gate_grad = lax.optimization_barrier((got, value_grad, gate_grad))
    weight_grad, mine = call(whole_kernel, (shape(8, CH), shape(16, CH)), [VMEM], (), cost(1))(got)
    other = lax.ppermute(mine, "c", ring(2, 1))
    taps_grad, gain_grad = call(
        last_kernel, (shape(KW, CH), shape(1, CH)), [VMEM, VMEM], (), cost(1)
    )(mine, other)
    return value_grad, gate_grad, taps_grad, gain_grad.reshape(CH), weight_grad


def solution(mesh):
    finer = Mesh(mesh.devices.reshape(16, 4, 2, mesh.shape["tp"]), ("z", "x", "c", "tp"))
    return jax.shard_map(
        body,
        mesh=finer,
        in_specs=(P(SP, "tp"), P(SP, "tp"), P(None, "tp"), P("tp"), P(None, "tp"), P(SP, "tp")),
        out_specs=(P(SP, "tp"), P(SP, "tp"), P(None, "tp"), P("tp"), P(SP, "tp")),
        check_vma=False,
    )
```

```python
import jax
import jax.numpy as jnp
from jax import lax
from jax.experimental import pallas as pl
from jax.experimental.pallas import tpu as pltpu
from jax.sharding import Mesh
from jax.sharding import PartitionSpec as P


GROUP = 64
SP = ("z", "x", "c")
EPS = 1e-06
ROWS = 1024
CH = 256
LANES = 128
PAD = 16
HALO = ROWS + 2 * PAD
KW = 31
F32 = jnp.float32
BF16 = jnp.bfloat16
CHUNK = 256
VMEM = pl.BlockSpec(memory_space=pltpu.VMEM)


def group_mean(x, avg):
    high = x.astype(BF16)
    low = (x - high.astype(F32)).astype(BF16)
    return jnp.dot(high, avg, preferred_element_type=F32) + jnp.dot(
        low, avg, preferred_element_type=F32
    )


def averaging():
    rows = lax.broadcasted_iota(jnp.int32, (CH, CH), 0) // GROUP
    cols = lax.broadcasted_iota(jnp.int32, (CH, CH), 1) // GROUP
    return jnp.where(rows == cols, 1.0 / GROUP, 0.0).astype(BF16)


def convolve(src, taps_at, store):
    tiles = 8
    for block in range(CH // LANES):

        def some_rows(step, _, block=block):
            start = pl.multiple_of(step * (8 * tiles), 8 * tiles)
            sums = [None] * tiles
            for k in range(KW):
                tap = taps_at(k, block)
                for j in range(tiles):
                    part = src[block, pl.ds(start + 8 * j + k + 1, 8), :] * tap
                    sums[j] = part if sums[j] is None else sums[j] + part
            for j in range(tiles):
                store(block, pl.multiple_of(start + 8 * j, 8), sums[j])
            return 0

        lax.fori_loop(0, ROWS // (8 * tiles), some_rows, 0)


def is_second():
    return lax.axis_index("c") == 1


def sides(second, inner, outer):
    return jnp.where(second, inner, outer), jnp.where(second, outer, inner)


def neighbours(inner, outer):
    second = is_second()
    before = jnp.where(second, inner[PAD : 2 * PAD].astype(F32), outer[PAD : 2 * PAD].astype(F32))
    after = jnp.where(second, outer[0:PAD].astype(F32), inner[0:PAD].astype(F32))
    return before, after


def edge_kernel(value_head, gate_head, value_tail, gate_tail, edges):
    def gated(value, gate):
        return (value[...].astype(F32) * jax.nn.sigmoid(gate[...].astype(F32))).astype(BF16)

    edges[0:PAD, :] = gated(value_head, gate_head)
    edges[PAD : 2 * PAD, :] = gated(value_tail, gate_tail)


def forward_kernel(
    value, gate, inner, outer, taps, gain, wide, unit, inv, slope, normed, conv
):
    lanes = [slice(b * LANES, (b + 1) * LANES) for b in range(2)]
    before, after = neighbours(inner, outer)
    for b in range(2):
        wide[b, 0:PAD, :] = before[:, lanes[b]]
        wide[b, PAD + ROWS : HALO, :] = after[:, lanes[b]]

    def gate_rows(step, _):
        start = pl.multiple_of(step * 64, 64)
        rows = pl.ds(start, 64)
        gated = (value[rows, :].astype(F32) * jax.nn.sigmoid(gate[rows, :].astype(F32))).astype(
            BF16
        )
        for b in range(2):
            wide[b, pl.ds(pl.multiple_of(start + PAD, 16), 64), :] = gated[:, lanes[b]].astype(F32)
        return 0

    lax.fori_loop(0, ROWS // 64, gate_rows, 0)

    def store(block, start, rows):
        conv[pl.ds(start, 8), lanes[block]] = rows

    lines = taps[...].astype(F32)
    convolve(
        wide, lambda k, b: jnp.broadcast_to(lines[k : k + 1, lanes[b]], (8, LANES)), store
    )
    avg = averaging()
    gain_row = gain[...]

    def norm_rows(step, _):
        rows = pl.ds(pl.multiple_of(step * CHUNK, CHUNK), CHUNK)
        raw = conv[rows, :]
        centred = raw - group_mean(raw, avg)
        scale = lax.rsqrt(group_mean(centred * centred, avg) + EPS)
        unit_rows = centred * scale
        pre = unit_rows * gain_row
        s = jax.nn.sigmoid(pre)
        unit[rows, :] = unit_rows
        inv[rows, :] = scale
        slope[rows, :] = s * (1.0 + pre * (1.0 - s))
        normed[rows, :] = (pre * s).astype(BF16)
        return 0

    lax.fori_loop(0, ROWS // CHUNK, norm_rows, 0)


def early_kernel(own, left, right, weight, normed, partial, wgrad):
    y = lax.axis_index("tp")
    blocks = ((own, lax.rem(y, 4)), (left, lax.rem(y + 3, 4)), (right, lax.rem(y + 1, 4)))
    weights = [weight[pl.ds(pl.multiple_of(at * CH, CH), CH), :] for _, at in blocks]

    def some_rows(step, _):
        rows = pl.ds(pl.multiple_of(step * CHUNK, CHUNK), CHUNK)
        total = None
        for (ref, _), w in zip(blocks, weights):
            part = jnp.dot(ref[rows, :], w, preferred_element_type=F32)
            total = part if total is None else total + part
        partial[rows, :] = total
        return 0

    lax.fori_loop(0, ROWS // CHUNK, some_rows, 0)
    for d, (ref, _) in enumerate(blocks):
        grads = lax.dot_general(
            ref[...], normed[...], (((0,), (0,)), ((), ())), preferred_element_type=F32
        )
        put_weight(wgrad, d, grads)


def put_weight(out, d, grads):
    pieces = grads.reshape(4, 8, 8, CH).astype(BF16)
    for near in range(4):
        for peer in range(8):
            out[peer, d * 4 + near] = pieces[near, peer]


def late_kernel(
    far, weight, normed, partial, unit, inv, slope, gain, wide, begun, grad, ends, sums
):
    y = lax.axis_index("tp")
    w = weight[pl.ds(pl.multiple_of(lax.rem(y + 2, 4) * CH, CH), CH), :]
    avg = averaging()
    gain_row = gain[...]

    def some_rows(step, gain_sum):
        start = pl.multiple_of(step * CHUNK, CHUNK)
        rows = pl.ds(start, CHUNK)
        normed_grad = partial[rows, :] + jnp.dot(far[rows, :], w, preferred_element_type=F32)
        u = unit[rows, :]
        act = normed_grad * slope[rows, :]
        au = act * u
        hat = act * gain_row
        hat_unit = au * gain_row
        rows_grad = inv[rows, :] * (
            hat - group_mean(hat, avg) - u * group_mean(hat_unit, avg)
        )
        for b in range(2):
            grad[b, rows, :] = rows_grad[:, b * LANES : (b + 1) * LANES]
        return gain_sum + jnp.sum(au.reshape(CHUNK // 8, 8, CH), axis=0)

    gain_sum = lax.fori_loop(0, ROWS // CHUNK, some_rows, jnp.zeros((8, CH), F32))
    for b in range(2):
        cols = slice(b * LANES, (b + 1) * LANES)
        ends[0:PAD, cols] = grad[b, 0:PAD, :]
        ends[PAD : 2 * PAD, cols] = grad[b, ROWS - PAD : ROWS, :]

    for peer in range(8):
        sums[peer, 0:12] = begun[peer]
    put_weight(
        sums,
        3,
        lax.dot_general(
            far[...], normed[...], (((0,), (0,)), ((), ())), preferred_element_type=F32
        ),
    )

    halves = []
    for b in range(2):
        lines = []
        for group in (range(0, 16), range(16, KW)):

            def tiles(step, carry, b=b, group=group):
                accs = list(carry)
                for j in range(4):
                    start = pl.multiple_of(step * 32, 32) + 8 * j
                    g = grad[b, pl.ds(start, 8), :]
                    for i, k in enumerate(group):
                        accs[i] = accs[i] + g * wide[b, pl.ds(start + k + 1, 8), :]
                return tuple(accs)

            accs = lax.fori_loop(
                0, ROWS // 32, tiles, tuple(jnp.zeros((8, LANES), F32) for _ in group)
            )
            lines += [jnp.sum(a, axis=0, keepdims=True) for a in accs]
        halves.append(jnp.concatenate(lines, axis=0))
    taps = jnp.concatenate(
        [
            jnp.concatenate(halves, axis=1),
            jnp.sum(gain_sum, axis=0, keepdims=True),
        ],
        axis=0,
    ).astype(BF16)
    for peer in range(8):
        for part in range(2):
            line = (peer % 2) * 16 + part * 8
            sums[peer, 16 + part] = taps[line : line + 8]


def backward_kernel(
    value, gate, grad, inner, outer, taps, value_grad, gate_grad, wide, conv
):
    before, after = neighbours(inner, outer)
    lines = taps[...].astype(F32)
    lanes = [slice(b * LANES, (b + 1) * LANES) for b in range(2)]
    for b in range(2):
        wide[b, 0:PAD, :] = before[:, lanes[b]]
        wide[b, PAD : PAD + ROWS, :] = grad[b]
        wide[b, PAD + ROWS : HALO, :] = after[:, lanes[b]]

    def store(block, start, rows):
        conv[pl.ds(start, 8), lanes[block]] = rows

    convolve(
        wide,
        lambda k, b: jnp.broadcast_to(lines[KW - 1 - k : KW - k, lanes[b]], (8, LANES)),
        store,
    )

    def finish(step, _):
        rows = pl.ds(pl.multiple_of(step * 64, 64), 64)
        s = jax.nn.sigmoid(gate[rows, :].astype(F32))
        down = conv[rows, :] * s
        value_grad[rows, :] = down.astype(BF16)
        gate_grad[rows, :] = (down * value[rows, :].astype(F32) * (1.0 - s)).astype(BF16)
        return 0

    lax.fori_loop(0, ROWS // 64, finish, 0)


def middle_kernel(late, out):
    y = lax.axis_index("tp")
    taps = late[0, 16:18].astype(F32)
    for peer in range(1, 8):
        taps = taps + late[peer, 16:18].astype(F32)
    taps = taps.astype(BF16)
    for d, at in enumerate((y, y + 3, y + 1, y + 2)):
        home = lax.rem(at, 4)
        for near in range(4):
            total = late[0, d * 4 + near].astype(F32)
            for peer in range(1, 8):
                total = total + late[peer, d * 4 + near].astype(F32)
            out[home * 4 + near, 0] = total.astype(BF16)
            out[home * 4 + near, 1:3] = taps


def whole_kernel(got, weight, mine):
    total = got[0].astype(F32)
    for peer in range(1, 16):
        total = total + got[peer].astype(F32)
    weight[...] = total[0]
    mine[0:8] = total[1]
    mine[8:16] = total[2]


def last_kernel(mine, other, taps, gain):
    low, high = sides(is_second(), other[...], mine[...])
    taps[0:16] = low
    taps[16:31] = high[:15]
    gain[...] = high[15:16]


def call(kernel, outs, specs, scratch=(), cost=None):
    return pl.pallas_call(
        kernel,
        out_shape=outs,
        in_specs=specs,
        out_specs=jax.tree.map(lambda _: VMEM, outs),
        scratch_shapes=scratch,
        cost_estimate=cost,
        compiler_params=pltpu.CompilerParams(vmem_limit_bytes=8 * 1024 * 1024),
    )


def shape(*dims, dtype=F32):
    return jax.ShapeDtypeStruct(dims, dtype)


def cost(us):
    return pl.CostEstimate(flops=int(us * 1e-6 * 2e14), bytes_accessed=2**20, transcendentals=0)


def ring(size, by):
    return [(i, (i + by) % size) for i in range(size)]


def body(value_rows, gate_rows, conv_taps, norm_gain, point_weight, out_grad):
    peers = lax.axis_size(SP)
    pairs = [(i, i ^ 1) for i in range(peers)]
    apart = [(i, i + 1) for i in range(1, peers - 1, 2)]
    apart = apart + [(j, i) for i, j in apart]
    gain = norm_gain.reshape(1, CH)

    def exchange(array, axis):
        return lax.all_to_all(array, axis, 0, 0, tiled=True)

    first_rows = pl.BlockSpec((PAD, CH), lambda i: (0, 0))
    last_rows = pl.BlockSpec((PAD, CH), lambda i: (ROWS // PAD - 1, 0))
    edges = pl.pallas_call(
        edge_kernel,
        out_shape=shape(2 * PAD, CH, dtype=BF16),
        grid=(1,),
        in_specs=[first_rows, first_rows, last_rows, last_rows],
        out_specs=pl.BlockSpec((2 * PAD, CH), lambda i: (0, 0)),
        name="edges",
    )(value_rows, gate_rows, value_rows, gate_rows)
    left = lax.ppermute(out_grad, "tp", ring(4, 1))
    right = lax.ppermute(out_grad, "tp", ring(4, 3))
    inner = lax.ppermute(edges, SP, pairs)
    outer = lax.ppermute(edges, SP, apart)
    far = lax.ppermute(out_grad, "tp", ring(4, 2))

    wide, unit, inv, slope, normed = call(
        forward_kernel,
        (
            shape(2, HALO, LANES),
            shape(ROWS, CH),
            shape(ROWS, CH),
            shape(ROWS, CH),
            shape(ROWS, CH, dtype=BF16),
        ),
        [VMEM] * 6,
        [pltpu.VMEM((ROWS, CH), F32)],
        cost(7),
    )(value_rows, gate_rows, inner, outer, conv_taps, gain)

    partial, wgrad = call(
        early_kernel, (shape(ROWS, CH), shape(8, 12, 8, CH, dtype=BF16)), [VMEM] * 5, (), cost(4)
    )(out_grad, left, right, point_weight, normed)

    grad, ends, sums = call(
        late_kernel,
        (
            shape(2, ROWS, LANES),
            shape(2 * PAD, CH),
            shape(8, 18, 8, CH, dtype=BF16),
        ),
        [VMEM] * 10,
        (),
        cost(8),
    )(far, point_weight, normed, partial, unit, inv, slope, gain, wide, wgrad)
    late = exchange(sums, ("x", "c"))

    inner = lax.ppermute(ends, SP, pairs)
    outer = lax.ppermute(ends, SP, apart)
    late, inner, outer = lax.optimization_barrier((late, inner, outer))
    sent = call(middle_kernel, shape(16, 3, 8, CH, dtype=BF16), [VMEM], (), cost(1))(late)
    got = exchange(sent, "z")

    value_grad, gate_grad = call(
        backward_kernel,
        (shape(ROWS, CH, dtype=BF16), shape(ROWS, CH, dtype=BF16)),
        [VMEM] * 6,
        [pltpu.VMEM((2, HALO, LANES), F32), pltpu.VMEM((ROWS, CH), F32)],
        cost(6),
    )(value_rows, gate_rows, grad, inner, outer, conv_taps)

    got, value_grad, gate_grad = lax.optimization_barrier((got, value_grad, gate_grad))
    weight_grad, mine = call(whole_kernel, (shape(8, CH), shape(16, CH)), [VMEM], (), cost(1))(got)
    other = lax.ppermute(mine, "c", ring(2, 1))
    taps_grad, gain_grad = call(
        last_kernel, (shape(KW, CH), shape(1, CH)), [VMEM, VMEM], (), cost(1)
    )(mine, other)
    return value_grad, gate_grad, taps_grad, gain_grad.reshape(CH), weight_grad


def solution(mesh):
    finer = Mesh(mesh.devices.reshape(16, 4, 2, mesh.shape["tp"]), ("z", "x", "c", "tp"))
    return jax.shard_map(
        body,
        mesh=finer,
        in_specs=(P(SP, "tp"), P(SP, "tp"), P(None, "tp"), P("tp"), P(None, "tp"), P(SP, "tp")),
        out_specs=(P(SP, "tp"), P(SP, "tp"), P(None, "tp"), P("tp"), P(SP, "tp")),
        check_vma=False,
    )
```

```python
import jax
import jax.numpy as jnp
from jax import lax
from jax.experimental import pallas as pl
from jax.experimental.pallas import tpu as pltpu
from jax.sharding import Mesh
from jax.sharding import PartitionSpec as P


GROUP = 64
SP = ("z", "x", "c")
EPS = 1e-06
ROWS = 1024
CH = 256
LANES = 128
PAD = 16
HALO = ROWS + 2 * PAD
KW = 31
F32 = jnp.float32
BF16 = jnp.bfloat16
CHUNK = 256
VMEM = pl.BlockSpec(memory_space=pltpu.VMEM)


def group_mean(x, avg):
    high = x.astype(BF16)
    low = (x - high.astype(F32)).astype(BF16)
    return jnp.dot(high, avg, preferred_element_type=F32) + jnp.dot(
        low, avg, preferred_element_type=F32
    )


def averaging():
    rows = lax.broadcasted_iota(jnp.int32, (CH, CH), 0) // GROUP
    cols = lax.broadcasted_iota(jnp.int32, (CH, CH), 1) // GROUP
    return jnp.where(rows == cols, 1.0 / GROUP, 0.0).astype(BF16)


def convolve(src, taps_at, store):
    tiles = 8
    for block in range(CH // LANES):

        def some_rows(step, _, block=block):
            start = pl.multiple_of(step * (8 * tiles), 8 * tiles)
            sums = [None] * tiles
            for k in range(KW):
                tap = taps_at(k, block)
                for j in range(tiles):
                    part = src[block, pl.ds(start + 8 * j + k + 1, 8), :] * tap
                    sums[j] = part if sums[j] is None else sums[j] + part
            for j in range(tiles):
                store(block, pl.multiple_of(start + 8 * j, 8), sums[j])
            return 0

        lax.fori_loop(0, ROWS // (8 * tiles), some_rows, 0)


def is_second():
    return lax.axis_index("c") == 1


def sides(second, inner, outer):
    return jnp.where(second, inner, outer), jnp.where(second, outer, inner)


def neighbours(inner, outer):
    second = is_second()
    before = jnp.where(second, inner[PAD : 2 * PAD].astype(F32), outer[PAD : 2 * PAD].astype(F32))
    after = jnp.where(second, outer[0:PAD].astype(F32), inner[0:PAD].astype(F32))
    return before, after


def edge_kernel(value_head, gate_head, value_tail, gate_tail, edges):
    def gated(value, gate):
        return (value[...].astype(F32) * jax.nn.sigmoid(gate[...].astype(F32))).astype(BF16)

    edges[0:PAD, :] = gated(value_head, gate_head)
    edges[PAD : 2 * PAD, :] = gated(value_tail, gate_tail)


def forward_kernel(
    value, gate, inner, outer, taps, gain, wide, unit, inv, slope, normed, conv
):
    lanes = [slice(b * LANES, (b + 1) * LANES) for b in range(2)]
    before, after = neighbours(inner, outer)
    for b in range(2):
        wide[b, 0:PAD, :] = before[:, lanes[b]]
        wide[b, PAD + ROWS : HALO, :] = after[:, lanes[b]]

    def gate_rows(step, _):
        start = pl.multiple_of(step * 64, 64)
        rows = pl.ds(start, 64)
        gated = (value[rows, :].astype(F32) * jax.nn.sigmoid(gate[rows, :].astype(F32))).astype(
            BF16
        )
        for b in range(2):
            wide[b, pl.ds(pl.multiple_of(start + PAD, 16), 64), :] = gated[:, lanes[b]].astype(F32)
        return 0

    lax.fori_loop(0, ROWS // 64, gate_rows, 0)

    def store(block, start, rows):
        conv[pl.ds(start, 8), lanes[block]] = rows

    lines = taps[...].astype(F32)
    convolve(
        wide, lambda k, b: jnp.broadcast_to(lines[k : k + 1, lanes[b]], (8, LANES)), store
    )
    avg = averaging()
    gain_row = gain[...]

    def norm_rows(step, _):
        rows = pl.ds(pl.multiple_of(step * CHUNK, CHUNK), CHUNK)
        raw = conv[rows, :]
        centred = raw - group_mean(raw, avg)
        scale = lax.rsqrt(group_mean(centred * centred, avg) + EPS)
        unit_rows = centred * scale
        pre = unit_rows * gain_row
        s = jax.nn.sigmoid(pre)
        unit[rows, :] = unit_rows
        inv[rows, :] = scale
        slope[rows, :] = s * (1.0 + pre * (1.0 - s))
        normed[rows, :] = (pre * s).astype(BF16)
        return 0

    lax.fori_loop(0, ROWS // CHUNK, norm_rows, 0)


def early_kernel(own, left, right, weight, normed, partial, kept, given):
    y = lax.axis_index("tp")
    blocks = ((own, lax.rem(y, 4)), (left, lax.rem(y + 3, 4)), (right, lax.rem(y + 1, 4)))
    weights = [weight[pl.ds(pl.multiple_of(at * CH, CH), CH), :] for _, at in blocks]

    def some_rows(step, _):
        rows = pl.ds(pl.multiple_of(step * CHUNK, CHUNK), CHUNK)
        total = None
        for (ref, _), w in zip(blocks, weights):
            part = jnp.dot(ref[rows, :], w, preferred_element_type=F32)
            total = part if total is None else total + part
        partial[rows, :] = total
        return 0

    lax.fori_loop(0, ROWS // CHUNK, some_rows, 0)
    for d, (ref, _) in enumerate(blocks):
        grads = lax.dot_general(
            ref[...], normed[...], (((0,), (0,)), ((), ())), preferred_element_type=F32
        )
        pieces = grads.reshape(4, 8, 8, CH).astype(BF16)
        for m in range(2):
            even, odd = pieces[2 * m], pieces[2 * m + 1]
            kept[:, d * 2 + m], given[:, d * 2 + m] = sides(is_second(), odd, even)


def late_kernel(
    far, weight, normed, partial, unit, inv, slope, gain, wide, kept, taken, grad, ends, sums
):
    y = lax.axis_index("tp")
    w = weight[pl.ds(pl.multiple_of(lax.rem(y + 2, 4) * CH, CH), CH), :]
    avg = averaging()
    gain_row = gain[...]

    def some_rows(step, gain_sum):
        start = pl.multiple_of(step * CHUNK, CHUNK)
        rows = pl.ds(start, CHUNK)
        normed_grad = partial[rows, :] + jnp.dot(far[rows, :], w, preferred_element_type=F32)
        u = unit[rows, :]
        act = normed_grad * slope[rows, :]
        au = act * u
        hat = act * gain_row
        hat_unit = au * gain_row
        rows_grad = inv[rows, :] * (
            hat - group_mean(hat, avg) - u * group_mean(hat_unit, avg)
        )
        for b in range(2):
            grad[b, rows, :] = rows_grad[:, b * LANES : (b + 1) * LANES]
        return gain_sum + jnp.sum(au.reshape(CHUNK // 8, 8, CH), axis=0)

    gain_sum = lax.fori_loop(0, ROWS // CHUNK, some_rows, jnp.zeros((8, CH), F32))
    for b in range(2):
        cols = slice(b * LANES, (b + 1) * LANES)
        ends[0:PAD, cols] = grad[b, 0:PAD, :]
        ends[PAD : 2 * PAD, cols] = grad[b, ROWS - PAD : ROWS, :]

    sums[:, 0:6] = (kept[...].astype(F32) + taken[...].astype(F32)).astype(BF16)
    pieces = lax.dot_general(
        far[...], normed[...], (((0,), (0,)), ((), ())), preferred_element_type=F32
    ).reshape(4, 8, 8, CH).astype(BF16)
    for near in range(4):
        sums[:, 6 + near] = pieces[near]

    halves = []
    for b in range(2):
        lines = []
        for group in (range(0, 16), range(16, KW)):

            def tiles(step, carry, b=b, group=group):
                accs = list(carry)
                for j in range(4):
                    start = pl.multiple_of(step * 32, 32) + 8 * j
                    g = grad[b, pl.ds(start, 8), :]
                    for i, k in enumerate(group):
                        accs[i] = accs[i] + g * wide[b, pl.ds(start + k + 1, 8), :]
                return tuple(accs)

            accs = lax.fori_loop(
                0, ROWS // 32, tiles, tuple(jnp.zeros((8, LANES), F32) for _ in group)
            )
            lines += [jnp.sum(a, axis=0, keepdims=True) for a in accs]
        halves.append(jnp.concatenate(lines, axis=0))
    taps = jnp.concatenate(
        [
            jnp.concatenate(halves, axis=1),
            jnp.sum(gain_sum, axis=0, keepdims=True),
        ],
        axis=0,
    ).astype(BF16)
    for peer in range(8):
        for part in range(2):
            line = (peer % 2) * 16 + part * 8
            sums[peer, 10 + part] = taps[line : line + 8]


def backward_kernel(
    value, gate, grad, inner, outer, taps, value_grad, gate_grad, wide, conv
):
    before, after = neighbours(inner, outer)
    lines = taps[...].astype(F32)
    lanes = [slice(b * LANES, (b + 1) * LANES) for b in range(2)]
    for b in range(2):
        wide[b, 0:PAD, :] = before[:, lanes[b]]
        wide[b, PAD : PAD + ROWS, :] = grad[b]
        wide[b, PAD + ROWS : HALO, :] = after[:, lanes[b]]

    def store(block, start, rows):
        conv[pl.ds(start, 8), lanes[block]] = rows

    convolve(
        wide,
        lambda k, b: jnp.broadcast_to(lines[KW - 1 - k : KW - k, lanes[b]], (8, LANES)),
        store,
    )

    def finish(step, _):
        rows = pl.ds(pl.multiple_of(step * 64, 64), 64)
        s = jax.nn.sigmoid(gate[rows, :].astype(F32))
        down = conv[rows, :] * s
        value_grad[rows, :] = down.astype(BF16)
        gate_grad[rows, :] = (down * value[rows, :].astype(F32) * (1.0 - s)).astype(BF16)
        return 0

    lax.fori_loop(0, ROWS // 64, finish, 0)


def middle_kernel(late, out):
    y = lax.axis_index("tp")

    def total(tile, peers):
        sums = None
        for peer in peers:
            part = late[peer, tile].astype(F32)
            sums = part if sums is None else sums + part
        return sums.astype(BF16)

    taps = [total(10 + part, range(8)) for part in range(2)]
    for d, at in enumerate((y, y + 3, y + 1, y + 2)):
        home = lax.rem(at, 4)
        for near in range(4):
            if d < 3:
                rows = total(d * 2 + near // 2, range(near % 2, 8, 2))
            else:
                rows = total(6 + near, range(8))
            out[home * 4 + near, 0] = rows
            for part in range(2):
                out[home * 4 + near, 1 + part] = taps[part]


def whole_kernel(got, weight, mine):
    total = got[0].astype(F32)
    for peer in range(1, 16):
        total = total + got[peer].astype(F32)
    weight[...] = total[0]
    mine[0:8] = total[1]
    mine[8:16] = total[2]


def last_kernel(mine, other, taps, gain):
    low, high = sides(is_second(), other[...], mine[...])
    taps[0:16] = low
    taps[16:31] = high[:15]
    gain[...] = high[15:16]


def call(kernel, outs, specs, scratch=(), cost=None):
    return pl.pallas_call(
        kernel,
        out_shape=outs,
        in_specs=specs,
        out_specs=jax.tree.map(lambda _: VMEM, outs),
        scratch_shapes=scratch,
        cost_estimate=cost,
        compiler_params=pltpu.CompilerParams(vmem_limit_bytes=8 * 1024 * 1024),
    )


def shape(*dims, dtype=F32):
    return jax.ShapeDtypeStruct(dims, dtype)


def cost(us):
    return pl.CostEstimate(flops=int(us * 1e-6 * 2e14), bytes_accessed=2**20, transcendentals=0)


def ring(size, by):
    return [(i, (i + by) % size) for i in range(size)]


def body(value_rows, gate_rows, conv_taps, norm_gain, point_weight, out_grad):
    peers = lax.axis_size(SP)
    pairs = [(i, i ^ 1) for i in range(peers)]
    apart = [(i, i + 1) for i in range(1, peers - 1, 2)]
    apart = apart + [(j, i) for i, j in apart]
    gain = norm_gain.reshape(1, CH)

    def exchange(array, axis):
        return lax.all_to_all(array, axis, 0, 0, tiled=True)

    first_rows = pl.BlockSpec((PAD, CH), lambda i: (0, 0))
    last_rows = pl.BlockSpec((PAD, CH), lambda i: (ROWS // PAD - 1, 0))
    edges = pl.pallas_call(
        edge_kernel,
        out_shape=shape(2 * PAD, CH, dtype=BF16),
        grid=(1,),
        in_specs=[first_rows, first_rows, last_rows, last_rows],
        out_specs=pl.BlockSpec((2 * PAD, CH), lambda i: (0, 0)),
        name="edges",
    )(value_rows, gate_rows, value_rows, gate_rows)
    left = lax.ppermute(out_grad, "tp", ring(4, 1))
    right = lax.ppermute(out_grad, "tp", ring(4, 3))
    inner = lax.ppermute(edges, SP, pairs)
    outer = lax.ppermute(edges, SP, apart)
    far = lax.ppermute(out_grad, "tp", ring(4, 2))

    wide, unit, inv, slope, normed = call(
        forward_kernel,
        (
            shape(2, HALO, LANES),
            shape(ROWS, CH),
            shape(ROWS, CH),
            shape(ROWS, CH),
            shape(ROWS, CH, dtype=BF16),
        ),
        [VMEM] * 6,
        [pltpu.VMEM((ROWS, CH), F32)],
        cost(7),
    )(value_rows, gate_rows, inner, outer, conv_taps, gain)

    half = shape(8, 6, 8, CH, dtype=BF16)
    partial, kept, given = call(
        early_kernel, (shape(ROWS, CH), half, half), [VMEM] * 5, (), cost(4)
    )(out_grad, left, right, point_weight, normed)

    taken = lax.ppermute(given, SP, pairs)

    grad, ends, sums = call(
        late_kernel,
        (
            shape(2, ROWS, LANES),
            shape(2 * PAD, CH),
            shape(8, 12, 8, CH, dtype=BF16),
        ),
        [VMEM] * 11,
        (),
        cost(8),
    )(far, point_weight, normed, partial, unit, inv, slope, gain, wide, kept, taken)
    late = exchange(sums, ("x", "c"))

    inner = lax.ppermute(ends, SP, pairs)
    outer = lax.ppermute(ends, SP, apart)
    late, inner, outer = lax.optimization_barrier((late, inner, outer))
    sent = call(middle_kernel, shape(16, 3, 8, CH, dtype=BF16), [VMEM], (), cost(1))(late)
    got = exchange(sent, "z")

    value_grad, gate_grad = call(
        backward_kernel,
        (shape(ROWS, CH, dtype=BF16), shape(ROWS, CH, dtype=BF16)),
        [VMEM] * 6,
        [pltpu.VMEM((2, HALO, LANES), F32), pltpu.VMEM((ROWS, CH), F32)],
        cost(6),
    )(value_rows, gate_rows, grad, inner, outer, conv_taps)

    got, value_grad, gate_grad = lax.optimization_barrier((got, value_grad, gate_grad))
    weight_grad, mine = call(whole_kernel, (shape(8, CH), shape(16, CH)), [VMEM], (), cost(1))(got)
    other = lax.ppermute(mine, "c", ring(2, 1))
    taps_grad, gain_grad = call(
        last_kernel, (shape(KW, CH), shape(1, CH)), [VMEM, VMEM], (), cost(1)
    )(mine, other)
    return value_grad, gate_grad, taps_grad, gain_grad.reshape(CH), weight_grad


def solution(mesh):
    finer = Mesh(mesh.devices.reshape(16, 4, 2, mesh.shape["tp"]), ("z", "x", "c", "tp"))
    return jax.shard_map(
        body,
        mesh=finer,
        in_specs=(P(SP, "tp"), P(SP, "tp"), P(None, "tp"), P("tp"), P(None, "tp"), P(SP, "tp")),
        out_specs=(P(SP, "tp"), P(SP, "tp"), P(None, "tp"), P("tp"), P(SP, "tp")),
        check_vma=False,
    )
```

```python
import functools

import jax
import jax.numpy as jnp
from jax import lax
from jax.experimental import pallas as pl
from jax.experimental.pallas import tpu as pltpu
from jax.sharding import Mesh
from jax.sharding import PartitionSpec as P


GROUP = 64
SP = ("z", "x", "c")
EPS = 1e-06
ROWS = 1024
CH = 256
LANES = 128
HALF = 512
PAD = 16
HALO = ROWS + 2 * PAD
KW = 31
F32 = jnp.float32
BF16 = jnp.bfloat16
CHUNK = 256
VMEM = pl.BlockSpec(memory_space=pltpu.VMEM)


def group_mean(x, avg):
    high = x.astype(BF16)
    low = (x - high.astype(F32)).astype(BF16)
    return jnp.dot(high, avg, preferred_element_type=F32) + jnp.dot(
        low, avg, preferred_element_type=F32
    )


def averaging():
    rows = lax.broadcasted_iota(jnp.int32, (CH, CH), 0) // GROUP
    cols = lax.broadcasted_iota(jnp.int32, (CH, CH), 1) // GROUP
    return jnp.where(rows == cols, 1.0 / GROUP, 0.0).astype(BF16)


def convolve(src, taps_at, store):
    tiles = 8
    for block in range(CH // LANES):

        def some_rows(step, _, block=block):
            start = pl.multiple_of(step * (8 * tiles), 8 * tiles)
            sums = [None] * tiles
            for k in range(KW):
                tap = taps_at(k, block)
                for j in range(tiles):
                    part = src[block, pl.ds(start + 8 * j + k + 1, 8), :] * tap
                    sums[j] = part if sums[j] is None else sums[j] + part
            for j in range(tiles):
                store(block, pl.multiple_of(start + 8 * j, 8), sums[j])
            return 0

        lax.fori_loop(0, ROWS // (8 * tiles), some_rows, 0)


def is_second():
    return lax.axis_index("c") == 1


def sides(second, inner, outer):
    return jnp.where(second, inner, outer), jnp.where(second, outer, inner)


def neighbours(inner, outer):
    second = is_second()
    before = jnp.where(second, inner[PAD : 2 * PAD].astype(F32), outer[PAD : 2 * PAD].astype(F32))
    after = jnp.where(second, outer[0:PAD].astype(F32), inner[0:PAD].astype(F32))
    return before, after


def edge_kernel(value_head, gate_head, value_tail, gate_tail, edges):
    def gated(value, gate):
        return (value[...].astype(F32) * jax.nn.sigmoid(gate[...].astype(F32))).astype(BF16)

    edges[0:PAD, :] = gated(value_head, gate_head)
    edges[PAD : 2 * PAD, :] = gated(value_tail, gate_tail)


def forward_kernel(
    value, gate, inner, outer, taps, gain, wide, unit, inv, slope, normed, conv
):
    lanes = [slice(b * LANES, (b + 1) * LANES) for b in range(2)]
    before, after = neighbours(inner, outer)
    for b in range(2):
        wide[b, 0:PAD, :] = before[:, lanes[b]]
        wide[b, PAD + ROWS : HALO, :] = after[:, lanes[b]]

    def gate_rows(step, _):
        start = pl.multiple_of(step * 64, 64)
        rows = pl.ds(start, 64)
        gated = (value[rows, :].astype(F32) * jax.nn.sigmoid(gate[rows, :].astype(F32))).astype(
            BF16
        )
        for b in range(2):
            wide[b, pl.ds(pl.multiple_of(start + PAD, 16), 64), :] = gated[:, lanes[b]].astype(F32)
        return 0

    lax.fori_loop(0, ROWS // 64, gate_rows, 0)

    def store(block, start, rows):
        conv[pl.ds(start, 8), lanes[block]] = rows

    lines = taps[...].astype(F32)
    convolve(
        wide, lambda k, b: jnp.broadcast_to(lines[k : k + 1, lanes[b]], (8, LANES)), store
    )
    avg = averaging()
    gain_row = gain[...]

    def norm_rows(step, _):
        rows = pl.ds(pl.multiple_of(step * CHUNK, CHUNK), CHUNK)
        raw = conv[rows, :]
        centred = raw - group_mean(raw, avg)
        scale = lax.rsqrt(group_mean(centred * centred, avg) + EPS)
        unit_rows = centred * scale
        pre = unit_rows * gain_row
        s = jax.nn.sigmoid(pre)
        unit[rows, :] = unit_rows
        inv[rows, :] = scale
        slope[rows, :] = s * (1.0 + pre * (1.0 - s))
        normed[rows, :] = (pre * s).astype(BF16)
        return 0

    lax.fori_loop(0, ROWS // CHUNK, norm_rows, 0)


def homes(y):
    return y, lax.bitwise_xor(y, 1), 3 - y, lax.bitwise_xor(y, 2)


def early_kernel(own, left, right, weight, normed, partial, kept, given):
    y = lax.axis_index("tp")
    blocks = tuple(zip((own, left, right), homes(y)))
    weights = [weight[pl.ds(pl.multiple_of(at * CH, CH), CH), :] for _, at in blocks]

    def some_rows(step, _):
        rows = pl.ds(pl.multiple_of(step * CHUNK, CHUNK), CHUNK)
        total = None
        for (ref, _), w in zip(blocks, weights):
            part = jnp.dot(ref[rows, :], w, preferred_element_type=F32)
            total = part if total is None else total + part
        partial[rows, :] = total
        return 0

    lax.fori_loop(0, ROWS // CHUNK, some_rows, 0)
    for d, (ref, _) in enumerate(blocks):
        grads = lax.dot_general(
            ref[...], normed[...], (((0,), (0,)), ((), ())), preferred_element_type=F32
        )
        pieces = grads.reshape(4, 8, 8, CH).astype(BF16)
        for m in range(2):
            even, odd = pieces[2 * m], pieces[2 * m + 1]
            kept[:, d * 2 + m], given[:, d * 2 + m] = sides(is_second(), odd, even)


def late_kernel(
    far_top, far_bottom, weight, normed, partial, unit, inv, slope, gain, wide, kept, taken, grad, ends, sums
):
    y = lax.axis_index("tp")
    w = weight[pl.ds(pl.multiple_of(homes(y)[3] * CH, CH), CH), :]
    avg = averaging()
    gain_row = gain[...]

    def some_rows(step, gain_sum, far, base):
        start = pl.multiple_of(step * CHUNK, CHUNK)
        rows = pl.ds(start + base, CHUNK)
        normed_grad = partial[rows, :] + jnp.dot(
            far[pl.ds(start, CHUNK), :], w, preferred_element_type=F32)
        u = unit[rows, :]
        act = normed_grad * slope[rows, :]
        au = act * u
        hat = act * gain_row
        hat_unit = au * gain_row
        rows_grad = inv[rows, :] * (
            hat - group_mean(hat, avg) - u * group_mean(hat_unit, avg)
        )
        for b in range(2):
            grad[b, rows, :] = rows_grad[:, b * LANES : (b + 1) * LANES]
        return gain_sum + jnp.sum(au.reshape(CHUNK // 8, 8, CH), axis=0)

    gain_sum = jnp.zeros((8, CH), F32)
    for far, base in ((far_top, 0), (far_bottom, HALF)):
        gain_sum = lax.fori_loop(
            0, HALF // CHUNK, functools.partial(some_rows, far=far, base=base), gain_sum
        )
    for b in range(2):
        cols = slice(b * LANES, (b + 1) * LANES)
        ends[0:PAD, cols] = grad[b, 0:PAD, :]
        ends[PAD : 2 * PAD, cols] = grad[b, ROWS - PAD : ROWS, :]

    sums[:, 0:6] = (kept[...].astype(F32) + taken[...].astype(F32)).astype(BF16)
    pieces = lax.dot_general(
        far_top[...], normed[0:HALF, :], (((0,), (0,)), ((), ())), preferred_element_type=F32
    ) + lax.dot_general(
        far_bottom[...], normed[HALF:ROWS, :], (((0,), (0,)), ((), ())), preferred_element_type=F32
    )
    pieces = pieces.reshape(4, 8, 8, CH).astype(BF16)
    for near in range(4):
        sums[:, 6 + near] = pieces[near]

    halves = []
    for b in range(2):
        lines = []
        for group in (range(0, 16), range(16, KW)):

            def tiles(step, carry, b=b, group=group):
                accs = list(carry)
                for j in range(4):
                    start = pl.multiple_of(step * 32, 32) + 8 * j
                    g = grad[b, pl.ds(start, 8), :]
                    for i, k in enumerate(group):
                        accs[i] = accs[i] + g * wide[b, pl.ds(start + k + 1, 8), :]
                return tuple(accs)

            accs = lax.fori_loop(
                0, ROWS // 32, tiles, tuple(jnp.zeros((8, LANES), F32) for _ in group)
            )
            lines += [jnp.sum(a, axis=0, keepdims=True) for a in accs]
        halves.append(jnp.concatenate(lines, axis=0))
    taps = jnp.concatenate(
        [
            jnp.concatenate(halves, axis=1),
            jnp.sum(gain_sum, axis=0, keepdims=True),
        ],
        axis=0,
    ).astype(BF16)
    for peer in range(8):
        for part in range(2):
            line = (peer % 2) * 16 + part * 8
            sums[peer, 10 + part] = taps[line : line + 8]


def backward_kernel(
    value, gate, grad, inner, outer, taps, value_grad, gate_grad, wide, conv
):
    before, after = neighbours(inner, outer)
    lines = taps[...].astype(F32)
    lanes = [slice(b * LANES, (b + 1) * LANES) for b in range(2)]
    for b in range(2):
        wide[b, 0:PAD, :] = before[:, lanes[b]]
        wide[b, PAD : PAD + ROWS, :] = grad[b]
        wide[b, PAD + ROWS : HALO, :] = after[:, lanes[b]]

    def store(block, start, rows):
        conv[pl.ds(start, 8), lanes[block]] = rows

    convolve(
        wide,
        lambda k, b: jnp.broadcast_to(lines[KW - 1 - k : KW - k, lanes[b]], (8, LANES)),
        store,
    )

    def finish(step, _):
        rows = pl.ds(pl.multiple_of(step * 64, 64), 64)
        s = jax.nn.sigmoid(gate[rows, :].astype(F32))
        down = conv[rows, :] * s
        value_grad[rows, :] = down.astype(BF16)
        gate_grad[rows, :] = (down * value[rows, :].astype(F32) * (1.0 - s)).astype(BF16)
        return 0

    lax.fori_loop(0, ROWS // 64, finish, 0)


def middle_kernel(late, out):
    y = lax.axis_index("tp")

    def total(tile, peers):
        sums = None
        for peer in peers:
            part = late[peer, tile].astype(F32)
            sums = part if sums is None else sums + part
        return sums.astype(BF16)

    taps = [total(10 + part, range(8)) for part in range(2)]
    for d, home in enumerate(homes(y)):
        for near in range(4):
            if d < 3:
                rows = total(d * 2 + near // 2, range(near % 2, 8, 2))
            else:
                rows = total(6 + near, range(8))
            out[home * 4 + near, 0] = rows
            for part in range(2):
                out[home * 4 + near, 1 + part] = taps[part]


def whole_kernel(got, weight, mine):
    total = got[0].astype(F32)
    for peer in range(1, 16):
        total = total + got[peer].astype(F32)
    weight[...] = total[0]
    mine[0:8] = total[1]
    mine[8:16] = total[2]


def last_kernel(mine, other, taps, gain):
    low, high = sides(is_second(), other[...], mine[...])
    taps[0:16] = low
    taps[16:31] = high[:15]
    gain[...] = high[15:16]


def call(kernel, outs, specs, scratch=(), cost=None):
    return pl.pallas_call(
        kernel,
        out_shape=outs,
        in_specs=specs,
        out_specs=jax.tree.map(lambda _: VMEM, outs),
        scratch_shapes=scratch,
        cost_estimate=cost,
        compiler_params=pltpu.CompilerParams(vmem_limit_bytes=8 * 1024 * 1024),
    )


def shape(*dims, dtype=F32):
    return jax.ShapeDtypeStruct(dims, dtype)


def cost(us):
    return pl.CostEstimate(flops=int(us * 1e-6 * 2e14), bytes_accessed=2**20, transcendentals=0)


def ring(size, by):
    return [(i, (i + by) % size) for i in range(size)]


def body(value_rows, gate_rows, conv_taps, norm_gain, point_weight, out_grad):
    peers = lax.axis_size(SP)
    pairs = [(i, i ^ 1) for i in range(peers)]
    apart = [(i, i + 1) for i in range(1, peers - 1, 2)]
    apart = apart + [(j, i) for i, j in apart]
    gain = norm_gain.reshape(1, CH)

    def exchange(array, axis):
        return lax.all_to_all(array, axis, 0, 0, tiled=True)

    first_rows = pl.BlockSpec((PAD, CH), lambda i: (0, 0))
    last_rows = pl.BlockSpec((PAD, CH), lambda i: (ROWS // PAD - 1, 0))
    edges = pl.pallas_call(
        edge_kernel,
        out_shape=shape(2 * PAD, CH, dtype=BF16),
        grid=(1,),
        in_specs=[first_rows, first_rows, last_rows, last_rows],
        out_specs=pl.BlockSpec((2 * PAD, CH), lambda i: (0, 0)),
        name="edges",
    )(value_rows, gate_rows, value_rows, gate_rows)
    beside = [(i, i ^ 1) for i in range(4)]
    around = [(i, 3 - i) for i in range(4)]
    left = lax.ppermute(out_grad, "tp", beside)
    right = lax.ppermute(out_grad, "tp", around)
    inner = lax.ppermute(edges, SP, pairs)
    outer = lax.ppermute(edges, SP, apart)
    far_top = lax.ppermute(left[:HALF], "tp", around)
    far_bottom = lax.ppermute(right[HALF:], "tp", beside)

    wide, unit, inv, slope, normed = call(
        forward_kernel,
        (
            shape(2, HALO, LANES),
            shape(ROWS, CH),
            shape(ROWS, CH),
            shape(ROWS, CH),
            shape(ROWS, CH, dtype=BF16),
        ),
        [VMEM] * 6,
        [pltpu.VMEM((ROWS, CH), F32)],
        cost(7),
    )(value_rows, gate_rows, inner, outer, conv_taps, gain)

    half = shape(8, 6, 8, CH, dtype=BF16)
    partial, kept, given = call(
        early_kernel, (shape(ROWS, CH), half, half), [VMEM] * 5, (), cost(4)
    )(out_grad, left, right, point_weight, normed)

    taken = lax.ppermute(given, SP, pairs)

    grad, ends, sums = call(
        late_kernel,
        (
            shape(2, ROWS, LANES),
            shape(2 * PAD, CH),
            shape(8, 12, 8, CH, dtype=BF16),
        ),
        [VMEM] * 12,
        (),
        cost(8),
    )(far_top, far_bottom, point_weight, normed, partial, unit, inv, slope, gain, wide, kept, taken)
    late = exchange(sums, ("x", "c"))

    inner = lax.ppermute(ends, SP, pairs)
    outer = lax.ppermute(ends, SP, apart)
    late, inner, outer = lax.optimization_barrier((late, inner, outer))
    sent = call(middle_kernel, shape(16, 3, 8, CH, dtype=BF16), [VMEM], (), cost(1))(late)
    got = exchange(sent, "z")

    value_grad, gate_grad = call(
        backward_kernel,
        (shape(ROWS, CH, dtype=BF16), shape(ROWS, CH, dtype=BF16)),
        [VMEM] * 6,
        [pltpu.VMEM((2, HALO, LANES), F32), pltpu.VMEM((ROWS, CH), F32)],
        cost(6),
    )(value_rows, gate_rows, grad, inner, outer, conv_taps)

    got, value_grad, gate_grad = lax.optimization_barrier((got, value_grad, gate_grad))
    weight_grad, mine = call(whole_kernel, (shape(8, CH), shape(16, CH)), [VMEM], (), cost(1))(got)
    other = lax.ppermute(mine, "c", ring(2, 1))
    taps_grad, gain_grad = call(
        last_kernel, (shape(KW, CH), shape(1, CH)), [VMEM, VMEM], (), cost(1)
    )(mine, other)
    return value_grad, gate_grad, taps_grad, gain_grad.reshape(CH), weight_grad


def solution(mesh):
    finer = Mesh(mesh.devices.reshape(16, 4, 2, mesh.shape["tp"]), ("z", "x", "c", "tp"))
    return jax.shard_map(
        body,
        mesh=finer,
        in_specs=(P(SP, "tp"), P(SP, "tp"), P(None, "tp"), P("tp"), P(None, "tp"), P(SP, "tp")),
        out_specs=(P(SP, "tp"), P(SP, "tp"), P(None, "tp"), P("tp"), P(SP, "tp")),
        check_vma=False,
    )
```

```python
import jax
import jax.numpy as jnp
from jax import lax
from jax.experimental import pallas as pl
from jax.experimental.pallas import tpu as pltpu
from jax.sharding import Mesh
from jax.sharding import PartitionSpec as P


GROUP = 64
SP = ("z", "x", "c")
EPS = 1e-06
ROWS = 1024
CH = 256
LANES = 128
PAD = 16
HALO = ROWS + 2 * PAD
KW = 31
F32 = jnp.float32
BF16 = jnp.bfloat16
CHUNK = 256
VMEM = pl.BlockSpec(memory_space=pltpu.VMEM)


def group_mean(x, avg):
    high = x.astype(BF16)
    low = (x - high.astype(F32)).astype(BF16)
    return jnp.dot(high, avg, preferred_element_type=F32) + jnp.dot(
        low, avg, preferred_element_type=F32
    )


def averaging():
    rows = lax.broadcasted_iota(jnp.int32, (CH, CH), 0) // GROUP
    cols = lax.broadcasted_iota(jnp.int32, (CH, CH), 1) // GROUP
    return jnp.where(rows == cols, 1.0 / GROUP, 0.0).astype(BF16)


def convolve(src, taps_at, store):
    tiles = 8
    for block in range(CH // LANES):

        def some_rows(step, _, block=block):
            start = pl.multiple_of(step * (8 * tiles), 8 * tiles)
            sums = [None] * tiles
            for k in range(KW):
                tap = taps_at(k, block)
                for j in range(tiles):
                    part = src[block, pl.ds(start + 8 * j + k + 1, 8), :] * tap
                    sums[j] = part if sums[j] is None else sums[j] + part
            for j in range(tiles):
                store(block, pl.multiple_of(start + 8 * j, 8), sums[j])
            return 0

        lax.fori_loop(0, ROWS // (8 * tiles), some_rows, 0)


def is_second():
    return lax.axis_index("c") == 1


def sides(second, inner, outer):
    return jnp.where(second, inner, outer), jnp.where(second, outer, inner)


def neighbours(inner, outer):
    second = is_second()
    before = jnp.where(second, inner[PAD : 2 * PAD].astype(F32), outer[PAD : 2 * PAD].astype(F32))
    after = jnp.where(second, outer[0:PAD].astype(F32), inner[0:PAD].astype(F32))
    return before, after


def edge_kernel(value_head, gate_head, value_tail, gate_tail, edges):
    def gated(value, gate):
        return (value[...].astype(F32) * jax.nn.sigmoid(gate[...].astype(F32))).astype(BF16)

    edges[0:PAD, :] = gated(value_head, gate_head)
    edges[PAD : 2 * PAD, :] = gated(value_tail, gate_tail)


def forward_kernel(
    value, gate, inner, outer, taps, gain, wide, unit, inv, slope, normed, conv
):
    lanes = [slice(b * LANES, (b + 1) * LANES) for b in range(2)]
    before, after = neighbours(inner, outer)
    for b in range(2):
        wide[b, 0:PAD, :] = before[:, lanes[b]]
        wide[b, PAD + ROWS : HALO, :] = after[:, lanes[b]]

    def gate_rows(step, _):
        start = pl.multiple_of(step * 64, 64)
        rows = pl.ds(start, 64)
        gated = (value[rows, :].astype(F32) * jax.nn.sigmoid(gate[rows, :].astype(F32))).astype(
            BF16
        )
        for b in range(2):
            wide[b, pl.ds(pl.multiple_of(start + PAD, 16), 64), :] = gated[:, lanes[b]].astype(F32)
        return 0

    lax.fori_loop(0, ROWS // 64, gate_rows, 0)

    def store(block, start, rows):
        conv[pl.ds(start, 8), lanes[block]] = rows

    lines = taps[...].astype(F32)
    convolve(
        wide, lambda k, b: jnp.broadcast_to(lines[k : k + 1, lanes[b]], (8, LANES)), store
    )
    avg = averaging()
    gain_row = gain[...]

    def norm_rows(step, _):
        rows = pl.ds(pl.multiple_of(step * CHUNK, CHUNK), CHUNK)
        raw = conv[rows, :]
        centred = raw - group_mean(raw, avg)
        scale = lax.rsqrt(group_mean(centred * centred, avg) + EPS)
        unit_rows = centred * scale
        pre = unit_rows * gain_row
        s = jax.nn.sigmoid(pre)
        unit[rows, :] = unit_rows
        inv[rows, :] = scale
        slope[rows, :] = s * (1.0 + pre * (1.0 - s))
        normed[rows, :] = (pre * s).astype(BF16)
        return 0

    lax.fori_loop(0, ROWS // CHUNK, norm_rows, 0)


def homes(y):
    return y, lax.bitwise_xor(y, 1), 3 - y, lax.bitwise_xor(y, 2)


def early_kernel(own, left, right, weight, normed, partial, kept, given):
    y = lax.axis_index("tp")
    blocks = tuple(zip((own, left, right), homes(y)))
    weights = [weight[pl.ds(pl.multiple_of(at * CH, CH), CH), :] for _, at in blocks]

    def some_rows(step, _):
        rows = pl.ds(pl.multiple_of(step * CHUNK, CHUNK), CHUNK)
        total = None
        for (ref, _), w in zip(blocks, weights):
            part = jnp.dot(ref[rows, :], w, preferred_element_type=F32)
            total = part if total is None else total + part
        partial[rows, :] = total
        return 0

    lax.fori_loop(0, ROWS // CHUNK, some_rows, 0)
    for d, (ref, _) in enumerate(blocks):
        grads = lax.dot_general(
            ref[...], normed[...], (((0,), (0,)), ((), ())), preferred_element_type=F32
        )
        pieces = grads.reshape(4, 8, 8, CH).astype(BF16)
        for m in range(2):
            even, odd = pieces[2 * m], pieces[2 * m + 1]
            kept[:, d * 2 + m], given[:, d * 2 + m] = sides(is_second(), odd, even)


def late_kernel(
    far, weight, normed, partial, unit, inv, slope, gain, wide, kept, taken, grad, ends, sums
):
    y = lax.axis_index("tp")
    w = weight[pl.ds(pl.multiple_of(homes(y)[3] * CH, CH), CH), :]
    avg = averaging()
    gain_row = gain[...]

    def some_rows(step, gain_sum):
        start = pl.multiple_of(step * CHUNK, CHUNK)
        rows = pl.ds(start, CHUNK)
        normed_grad = partial[rows, :] + jnp.dot(far[rows, :], w, preferred_element_type=F32)
        u = unit[rows, :]
        act = normed_grad * slope[rows, :]
        au = act * u
        hat = act * gain_row
        hat_unit = au * gain_row
        rows_grad = inv[rows, :] * (
            hat - group_mean(hat, avg) - u * group_mean(hat_unit, avg)
        )
        for b in range(2):
            grad[b, rows, :] = rows_grad[:, b * LANES : (b + 1) * LANES]
        return gain_sum + jnp.sum(au.reshape(CHUNK // 8, 8, CH), axis=0)

    gain_sum = lax.fori_loop(0, ROWS // CHUNK, some_rows, jnp.zeros((8, CH), F32))
    for b in range(2):
        cols = slice(b * LANES, (b + 1) * LANES)
        ends[0:PAD, cols] = grad[b, 0:PAD, :]
        ends[PAD : 2 * PAD, cols] = grad[b, ROWS - PAD : ROWS, :]

    sums[:, 0:6] = (kept[...].astype(F32) + taken[...].astype(F32)).astype(BF16)
    pieces = lax.dot_general(
        far[...], normed[...], (((0,), (0,)), ((), ())), preferred_element_type=F32
    ).reshape(4, 8, 8, CH).astype(BF16)
    for near in range(4):
        sums[:, 6 + near] = pieces[near]

    halves = []
    for b in range(2):
        lines = []
        for group in (range(0, 16), range(16, KW)):

            def tiles(step, carry, b=b, group=group):
                accs = list(carry)
                for j in range(4):
                    start = pl.multiple_of(step * 32, 32) + 8 * j
                    g = grad[b, pl.ds(start, 8), :]
                    for i, k in enumerate(group):
                        accs[i] = accs[i] + g * wide[b, pl.ds(start + k + 1, 8), :]
                return tuple(accs)

            accs = lax.fori_loop(
                0, ROWS // 32, tiles, tuple(jnp.zeros((8, LANES), F32) for _ in group)
            )
            lines += [jnp.sum(a, axis=0, keepdims=True) for a in accs]
        halves.append(jnp.concatenate(lines, axis=0))
    taps = jnp.concatenate(
        [
            jnp.concatenate(halves, axis=1),
            jnp.sum(gain_sum, axis=0, keepdims=True),
        ],
        axis=0,
    ).astype(BF16)
    for peer in range(8):
        for part in range(2):
            line = (peer % 2) * 16 + part * 8
            sums[peer, 10 + part] = taps[line : line + 8]


def backward_kernel(
    value, gate, grad, inner, outer, taps, value_grad, gate_grad, wide, conv
):
    before, after = neighbours(inner, outer)
    lines = taps[...].astype(F32)
    lanes = [slice(b * LANES, (b + 1) * LANES) for b in range(2)]
    for b in range(2):
        wide[b, 0:PAD, :] = before[:, lanes[b]]
        wide[b, PAD : PAD + ROWS, :] = grad[b]
        wide[b, PAD + ROWS : HALO, :] = after[:, lanes[b]]

    def store(block, start, rows):
        conv[pl.ds(start, 8), lanes[block]] = rows

    convolve(
        wide,
        lambda k, b: jnp.broadcast_to(lines[KW - 1 - k : KW - k, lanes[b]], (8, LANES)),
        store,
    )

    def finish(step, _):
        rows = pl.ds(pl.multiple_of(step * 64, 64), 64)
        s = jax.nn.sigmoid(gate[rows, :].astype(F32))
        down = conv[rows, :] * s
        value_grad[rows, :] = down.astype(BF16)
        gate_grad[rows, :] = (down * value[rows, :].astype(F32) * (1.0 - s)).astype(BF16)
        return 0

    lax.fori_loop(0, ROWS // 64, finish, 0)


def middle_kernel(late, out):
    y = lax.axis_index("tp")

    def total(tile, peers):
        sums = None
        for peer in peers:
            part = late[peer, tile].astype(F32)
            sums = part if sums is None else sums + part
        return sums.astype(BF16)

    taps = [total(10 + part, range(8)) for part in range(2)]
    for d, home in enumerate(homes(y)):
        for near in range(4):
            if d < 3:
                rows = total(d * 2 + near // 2, range(near % 2, 8, 2))
            else:
                rows = total(6 + near, range(8))
            out[home * 4 + near, 0] = rows
            for part in range(2):
                out[home * 4 + near, 1 + part] = taps[part]


def whole_kernel(got, weight, mine):
    total = got[0].astype(F32)
    for peer in range(1, 16):
        total = total + got[peer].astype(F32)
    weight[...] = total[0]
    mine[0:8] = total[1]
    mine[8:16] = total[2]


def last_kernel(mine, other, taps, gain):
    low, high = sides(is_second(), other[...], mine[...])
    taps[0:16] = low
    taps[16:31] = high[:15]
    gain[...] = high[15:16]


def call(kernel, outs, specs, scratch=(), cost=None):
    return pl.pallas_call(
        kernel,
        out_shape=outs,
        in_specs=specs,
        out_specs=jax.tree.map(lambda _: VMEM, outs),
        scratch_shapes=scratch,
        cost_estimate=cost,
        compiler_params=pltpu.CompilerParams(vmem_limit_bytes=8 * 1024 * 1024),
    )


def shape(*dims, dtype=F32):
    return jax.ShapeDtypeStruct(dims, dtype)


def cost(us):
    return pl.CostEstimate(flops=int(us * 1e-6 * 2e14), bytes_accessed=2**20, transcendentals=0)


def ring(size, by):
    return [(i, (i + by) % size) for i in range(size)]


def body(value_rows, gate_rows, conv_taps, norm_gain, point_weight, out_grad):
    peers = lax.axis_size(SP)
    pairs = [(i, i ^ 1) for i in range(peers)]
    apart = [(i, i + 1) for i in range(1, peers - 1, 2)]
    apart = apart + [(j, i) for i, j in apart]
    gain = norm_gain.reshape(1, CH)

    def exchange(array, axis):
        return lax.all_to_all(array, axis, 0, 0, tiled=True)

    first_rows = pl.BlockSpec((PAD, CH), lambda i: (0, 0))
    last_rows = pl.BlockSpec((PAD, CH), lambda i: (ROWS // PAD - 1, 0))
    edges = pl.pallas_call(
        edge_kernel,
        out_shape=shape(2 * PAD, CH, dtype=BF16),
        grid=(1,),
        in_specs=[first_rows, first_rows, last_rows, last_rows],
        out_specs=pl.BlockSpec((2 * PAD, CH), lambda i: (0, 0)),
        name="edges",
    )(value_rows, gate_rows, value_rows, gate_rows)
    left = lax.ppermute(out_grad, "tp", [(i, i ^ 1) for i in range(4)])
    right = lax.ppermute(out_grad, "tp", [(i, 3 - i) for i in range(4)])
    inner = lax.ppermute(edges, SP, pairs)
    outer = lax.ppermute(edges, SP, apart)
    far = lax.ppermute(out_grad, "tp", [(i, i ^ 2) for i in range(4)])

    wide, unit, inv, slope, normed = call(
        forward_kernel,
        (
            shape(2, HALO, LANES),
            shape(ROWS, CH),
            shape(ROWS, CH),
            shape(ROWS, CH),
            shape(ROWS, CH, dtype=BF16),
        ),
        [VMEM] * 6,
        [pltpu.VMEM((ROWS, CH), F32)],
        cost(7),
    )(value_rows, gate_rows, inner, outer, conv_taps, gain)

    half = shape(8, 6, 8, CH, dtype=BF16)
    partial, kept, given = call(
        early_kernel, (shape(ROWS, CH), half, half), [VMEM] * 5, (), cost(4)
    )(out_grad, left, right, point_weight, normed)

    taken = lax.ppermute(given, SP, pairs)

    grad, ends, sums = call(
        late_kernel,
        (
            shape(2, ROWS, LANES),
            shape(2 * PAD, CH),
            shape(8, 12, 8, CH, dtype=BF16),
        ),
        [VMEM] * 11,
        (),
        cost(8),
    )(far, point_weight, normed, partial, unit, inv, slope, gain, wide, kept, taken)
    late = exchange(sums, ("x", "c"))

    inner = lax.ppermute(ends, SP, pairs)
    outer = lax.ppermute(ends, SP, apart)
    late, inner, outer = lax.optimization_barrier((late, inner, outer))
    sent = call(middle_kernel, shape(16, 3, 8, CH, dtype=BF16), [VMEM], (), cost(1))(late)
    got = exchange(sent, "z")

    value_grad, gate_grad = call(
        backward_kernel,
        (shape(ROWS, CH, dtype=BF16), shape(ROWS, CH, dtype=BF16)),
        [VMEM] * 6,
        [pltpu.VMEM((2, HALO, LANES), F32), pltpu.VMEM((ROWS, CH), F32)],
        cost(6),
    )(value_rows, gate_rows, grad, inner, outer, conv_taps)

    got, value_grad, gate_grad = lax.optimization_barrier((got, value_grad, gate_grad))
    weight_grad, mine = call(whole_kernel, (shape(8, CH), shape(16, CH)), [VMEM], (), cost(1))(got)
    other = lax.ppermute(mine, "c", ring(2, 1))
    taps_grad, gain_grad = call(
        last_kernel, (shape(KW, CH), shape(1, CH)), [VMEM, VMEM], (), cost(1)
    )(mine, other)
    return value_grad, gate_grad, taps_grad, gain_grad.reshape(CH), weight_grad


def solution(mesh):
    finer = Mesh(mesh.devices.reshape(16, 4, 2, mesh.shape["tp"]), ("z", "x", "c", "tp"))
    return jax.shard_map(
        body,
        mesh=finer,
        in_specs=(P(SP, "tp"), P(SP, "tp"), P(None, "tp"), P("tp"), P(None, "tp"), P(SP, "tp")),
        out_specs=(P(SP, "tp"), P(SP, "tp"), P(None, "tp"), P("tp"), P(SP, "tp")),
        check_vma=False,
    )
```

```python
import functools

import jax
import jax.numpy as jnp
from jax import lax
from jax.experimental import pallas as pl
from jax.experimental.pallas import tpu as pltpu
from jax.sharding import Mesh
from jax.sharding import PartitionSpec as P


GROUP = 64
SP = ("z", "x", "c")
EPS = 1e-06
ROWS = 1024
CH = 256
LANES = 128
HALF = 512
PAD = 16
HALO = ROWS + 2 * PAD
KW = 31
F32 = jnp.float32
BF16 = jnp.bfloat16
CHUNK = 256
VMEM = pl.BlockSpec(memory_space=pltpu.VMEM)


def group_mean(x, avg):
    high = x.astype(BF16)
    low = (x - high.astype(F32)).astype(BF16)
    return jnp.dot(high, avg, preferred_element_type=F32) + jnp.dot(
        low, avg, preferred_element_type=F32
    )


def rounded_mean(x, avg):
    return jnp.dot(x.astype(BF16), avg, preferred_element_type=F32)


def averaging():
    rows = lax.broadcasted_iota(jnp.int32, (CH, CH), 0) // GROUP
    cols = lax.broadcasted_iota(jnp.int32, (CH, CH), 1) // GROUP
    return jnp.where(rows == cols, 1.0 / GROUP, 0.0).astype(BF16)


def convolve(src, taps_at, store):
    tiles = 8
    for block in range(CH // LANES):

        def some_rows(step, _, block=block):
            start = pl.multiple_of(step * (8 * tiles), 8 * tiles)
            sums = [None] * tiles
            for k in range(KW):
                tap = taps_at(k, block)
                for j in range(tiles):
                    part = src[block, pl.ds(start + 8 * j + k + 1, 8), :] * tap
                    sums[j] = part if sums[j] is None else sums[j] + part
            for j in range(tiles):
                store(block, pl.multiple_of(start + 8 * j, 8), sums[j])
            return 0

        lax.fori_loop(0, ROWS // (8 * tiles), some_rows, 0)


def is_second():
    return lax.axis_index("c") == 1


def sides(second, inner, outer):
    return jnp.where(second, inner, outer), jnp.where(second, outer, inner)


def neighbours(inner, outer):
    second = is_second()
    before = jnp.where(second, inner[PAD : 2 * PAD].astype(F32), outer[PAD : 2 * PAD].astype(F32))
    after = jnp.where(second, outer[0:PAD].astype(F32), inner[0:PAD].astype(F32))
    return before, after


def edge_kernel(value_head, gate_head, value_tail, gate_tail, edges):
    def gated(value, gate):
        return (value[...].astype(F32) * jax.nn.sigmoid(gate[...].astype(F32))).astype(BF16)

    edges[0:PAD, :] = gated(value_head, gate_head)
    edges[PAD : 2 * PAD, :] = gated(value_tail, gate_tail)


def forward_kernel(
    value, gate, inner, outer, taps, gain, wide, unit, inv, slope, normed, conv
):
    lanes = [slice(b * LANES, (b + 1) * LANES) for b in range(2)]
    before, after = neighbours(inner, outer)
    for b in range(2):
        wide[b, 0:PAD, :] = before[:, lanes[b]]
        wide[b, PAD + ROWS : HALO, :] = after[:, lanes[b]]

    def gate_rows(step, _):
        start = pl.multiple_of(step * 64, 64)
        rows = pl.ds(start, 64)
        gated = (value[rows, :].astype(F32) * jax.nn.sigmoid(gate[rows, :].astype(F32))).astype(
            BF16
        )
        for b in range(2):
            wide[b, pl.ds(pl.multiple_of(start + PAD, 16), 64), :] = gated[:, lanes[b]].astype(F32)
        return 0

    lax.fori_loop(0, ROWS // 64, gate_rows, 0)

    def store(block, start, rows):
        conv[pl.ds(start, 8), lanes[block]] = rows

    lines = taps[...].astype(F32)
    convolve(
        wide, lambda k, b: jnp.broadcast_to(lines[k : k + 1, lanes[b]], (8, LANES)), store
    )
    avg = averaging()
    gain_row = gain[...]

    def norm_rows(step, _):
        rows = pl.ds(pl.multiple_of(step * CHUNK, CHUNK), CHUNK)
        raw = conv[rows, :]
        centred = raw - group_mean(raw, avg)
        scale = lax.rsqrt(rounded_mean(centred * centred, avg) + EPS)
        unit_rows = centred * scale
        pre = unit_rows * gain_row
        s = jax.nn.sigmoid(pre)
        unit[rows, :] = unit_rows
        inv[rows, :] = scale
        slope[rows, :] = s * (1.0 + pre * (1.0 - s))
        normed[rows, :] = (pre * s).astype(BF16)
        return 0

    lax.fori_loop(0, ROWS // CHUNK, norm_rows, 0)


def homes(y):
    return y, lax.bitwise_xor(y, 1), 3 - y, lax.bitwise_xor(y, 2)


def late_kernel(
    own, left, right, far_top, far_bottom, weight, normed, unit, inv, slope, gain, wide, grad, ends, sums
):
    y = lax.axis_index("tp")
    weights = [weight[pl.ds(pl.multiple_of(at * CH, CH), CH), :] for at in homes(y)]
    avg = averaging()
    gain_row = gain[...]

    def some_rows(step, gain_sum, far, base):
        start = pl.multiple_of(step * CHUNK, CHUNK)
        rows = pl.ds(start + base, CHUNK)
        normed_grad = jnp.dot(far[pl.ds(start, CHUNK), :], weights[3], preferred_element_type=F32)
        for ref, w in zip((own, left, right), weights):
            normed_grad = normed_grad + jnp.dot(ref[rows, :], w, preferred_element_type=F32)
        u = unit[rows, :]
        act = normed_grad * slope[rows, :]
        au = act * u
        hat = act * gain_row
        hat_unit = au * gain_row
        rows_grad = inv[rows, :] * (
            hat - group_mean(hat, avg) - u * rounded_mean(hat_unit, avg)
        )
        for b in range(2):
            grad[b, rows, :] = rows_grad[:, b * LANES : (b + 1) * LANES]
        return gain_sum + jnp.sum(au.reshape(CHUNK // 8, 8, CH), axis=0)

    gain_sum = jnp.zeros((8, CH), F32)
    for far, base in ((far_top, 0), (far_bottom, HALF)):
        gain_sum = lax.fori_loop(
            0, HALF // CHUNK, functools.partial(some_rows, far=far, base=base), gain_sum
        )
    for b in range(2):
        cols = slice(b * LANES, (b + 1) * LANES)
        ends[0:PAD, cols] = grad[b, 0:PAD, :]
        ends[PAD : 2 * PAD, cols] = grad[b, ROWS - PAD : ROWS, :]

    def against(block, start, size):
        return lax.dot_general(
            block[...],
            normed[start : start + size, :],
            (((0,), (0,)), ((), ())),
            preferred_element_type=F32,
        )

    for d, block in enumerate((own, left, right, None)):
        if block is None:
            grads = against(far_top, 0, HALF) + against(far_bottom, HALF, HALF)
        else:
            grads = against(block, 0, ROWS)
        pieces = grads.reshape(4, 8, 8, CH).astype(BF16)
        for near in range(4):
            sums[:, d * 4 + near] = pieces[near]

    halves = []
    for b in range(2):
        lines = []
        for group in (range(0, 16), range(16, KW)):

            def tiles(step, carry, b=b, group=group):
                accs = list(carry)
                for j in range(4):
                    start = pl.multiple_of(step * 32, 32) + 8 * j
                    g = grad[b, pl.ds(start, 8), :]
                    for i, k in enumerate(group):
                        accs[i] = accs[i] + g * wide[b, pl.ds(start + k + 1, 8), :]
                return tuple(accs)

            accs = lax.fori_loop(
                0, ROWS // 32, tiles, tuple(jnp.zeros((8, LANES), F32) for _ in group)
            )
            lines += [jnp.sum(a, axis=0, keepdims=True) for a in accs]
        halves.append(jnp.concatenate(lines, axis=0))
    taps = jnp.concatenate(
        [
            jnp.concatenate(halves, axis=1),
            jnp.sum(gain_sum, axis=0, keepdims=True),
        ],
        axis=0,
    ).astype(BF16)
    for peer in range(8):
        for part in range(2):
            line = (peer % 2) * 16 + part * 8
            sums[peer, 16 + part] = taps[line : line + 8]


def backward_kernel(
    value, gate, grad, inner, outer, taps, value_grad, gate_grad, wide, conv
):
    before, after = neighbours(inner, outer)
    lines = taps[...].astype(F32)
    lanes = [slice(b * LANES, (b + 1) * LANES) for b in range(2)]
    for b in range(2):
        wide[b, 0:PAD, :] = before[:, lanes[b]]
        wide[b, PAD : PAD + ROWS, :] = grad[b]
        wide[b, PAD + ROWS : HALO, :] = after[:, lanes[b]]

    def store(block, start, rows):
        conv[pl.ds(start, 8), lanes[block]] = rows

    convolve(
        wide,
        lambda k, b: jnp.broadcast_to(lines[KW - 1 - k : KW - k, lanes[b]], (8, LANES)),
        store,
    )

    def finish(step, _):
        rows = pl.ds(pl.multiple_of(step * 64, 64), 64)
        s = jax.nn.sigmoid(gate[rows, :].astype(F32))
        down = conv[rows, :] * s
        value_grad[rows, :] = down.astype(BF16)
        gate_grad[rows, :] = (down * value[rows, :].astype(F32) * (1.0 - s)).astype(BF16)
        return 0

    lax.fori_loop(0, ROWS // 64, finish, 0)


def middle_kernel(late, out):
    y = lax.axis_index("tp")

    def total(tile):
        sums = late[0, tile].astype(F32)
        for peer in range(1, 8):
            sums = sums + late[peer, tile].astype(F32)
        return sums.astype(BF16)

    taps = [total(16 + part) for part in range(2)]
    for d, home in enumerate(homes(y)):
        for near in range(4):
            out[home * 4 + near, 0] = total(d * 4 + near)
            for part in range(2):
                out[home * 4 + near, 1 + part] = taps[part]


def whole_kernel(got, weight, mine):
    total = got[0].astype(F32)
    for peer in range(1, 16):
        total = total + got[peer].astype(F32)
    weight[...] = total[0]
    mine[0:8] = total[1]
    mine[8:16] = total[2]


def last_kernel(mine, other, taps, gain):
    low, high = sides(is_second(), other[...], mine[...])
    taps[0:16] = low
    taps[16:31] = high[:15]
    gain[...] = high[15:16]


def call(kernel, outs, specs, scratch=(), cost=None):
    return pl.pallas_call(
        kernel,
        out_shape=outs,
        in_specs=specs,
        out_specs=jax.tree.map(lambda _: VMEM, outs),
        scratch_shapes=scratch,
        cost_estimate=cost,
        compiler_params=pltpu.CompilerParams(vmem_limit_bytes=8 * 1024 * 1024),
    )


def shape(*dims, dtype=F32):
    return jax.ShapeDtypeStruct(dims, dtype)


def cost(us):
    return pl.CostEstimate(flops=int(us * 1e-6 * 2e14), bytes_accessed=2**20, transcendentals=0)


def ring(size, by):
    return [(i, (i + by) % size) for i in range(size)]


def body(value_rows, gate_rows, conv_taps, norm_gain, point_weight, out_grad):
    peers = lax.axis_size(SP)
    pairs = [(i, i ^ 1) for i in range(peers)]
    apart = [(i, i + 1) for i in range(1, peers - 1, 2)]
    apart = apart + [(j, i) for i, j in apart]
    gain = norm_gain.reshape(1, CH)

    def exchange(array, axis):
        return lax.all_to_all(array, axis, 0, 0, tiled=True)

    first_rows = pl.BlockSpec((PAD, CH), lambda i: (0, 0))
    last_rows = pl.BlockSpec((PAD, CH), lambda i: (ROWS // PAD - 1, 0))
    edges = pl.pallas_call(
        edge_kernel,
        out_shape=shape(2 * PAD, CH, dtype=BF16),
        grid=(1,),
        in_specs=[first_rows, first_rows, last_rows, last_rows],
        out_specs=pl.BlockSpec((2 * PAD, CH), lambda i: (0, 0)),
        name="edges",
    )(value_rows, gate_rows, value_rows, gate_rows)
    beside = [(i, i ^ 1) for i in range(4)]
    around = [(i, 3 - i) for i in range(4)]
    left = lax.ppermute(out_grad, "tp", beside)
    right = lax.ppermute(out_grad, "tp", around)
    inner = lax.ppermute(edges, SP, pairs)
    outer = lax.ppermute(edges, SP, apart)
    far_top = lax.ppermute(left[:HALF], "tp", around)
    far_bottom = lax.ppermute(right[HALF:], "tp", beside)

    wide, unit, inv, slope, normed = call(
        forward_kernel,
        (
            shape(2, HALO, LANES),
            shape(ROWS, CH),
            shape(ROWS, CH),
            shape(ROWS, CH),
            shape(ROWS, CH, dtype=BF16),
        ),
        [VMEM] * 6,
        [pltpu.VMEM((ROWS, CH), F32)],
        cost(7),
    )(value_rows, gate_rows, inner, outer, conv_taps, gain)

    grad, ends, sums = call(
        late_kernel,
        (
            shape(2, ROWS, LANES),
            shape(2 * PAD, CH),
            shape(8, 18, 8, CH, dtype=BF16),
        ),
        [VMEM] * 12,
        (),
        cost(8),
    )(
        out_grad,
        left,
        right,
        far_top,
        far_bottom,
        point_weight,
        normed,
        unit,
        inv,
        slope,
        gain,
        wide,
    )
    late = exchange(sums, ("x", "c"))

    inner = lax.ppermute(ends, SP, pairs)
    outer = lax.ppermute(ends, SP, apart)
    late, inner, outer = lax.optimization_barrier((late, inner, outer))
    sent = call(middle_kernel, shape(16, 3, 8, CH, dtype=BF16), [VMEM], (), cost(1))(late)
    got = exchange(sent, "z")

    value_grad, gate_grad = call(
        backward_kernel,
        (shape(ROWS, CH, dtype=BF16), shape(ROWS, CH, dtype=BF16)),
        [VMEM] * 6,
        [pltpu.VMEM((2, HALO, LANES), F32), pltpu.VMEM((ROWS, CH), F32)],
        cost(6),
    )(value_rows, gate_rows, grad, inner, outer, conv_taps)

    got, value_grad, gate_grad = lax.optimization_barrier((got, value_grad, gate_grad))
    weight_grad, mine = call(whole_kernel, (shape(8, CH), shape(16, CH)), [VMEM], (), cost(1))(got)
    other = lax.ppermute(mine, "c", ring(2, 1))
    taps_grad, gain_grad = call(
        last_kernel, (shape(KW, CH), shape(1, CH)), [VMEM, VMEM], (), cost(1)
    )(mine, other)
    return value_grad, gate_grad, taps_grad, gain_grad.reshape(CH), weight_grad


def solution(mesh):
    finer = Mesh(mesh.devices.reshape(16, 4, 2, mesh.shape["tp"]), ("z", "x", "c", "tp"))
    return jax.shard_map(
        body,
        mesh=finer,
        in_specs=(P(SP, "tp"), P(SP, "tp"), P(None, "tp"), P("tp"), P(None, "tp"), P(SP, "tp")),
        out_specs=(P(SP, "tp"), P(SP, "tp"), P(None, "tp"), P("tp"), P(SP, "tp")),
        check_vma=False,
    )
```

```python
import functools

import jax
import jax.numpy as jnp
from jax import lax
from jax.experimental import pallas as pl
from jax.experimental.pallas import tpu as pltpu
from jax.sharding import Mesh
from jax.sharding import PartitionSpec as P


GROUP = 64
SP = ("z", "x", "c")
EPS = 1e-06
ROWS = 1024
CH = 256
LANES = 128
HALF = 512
PAD = 16
HALO = ROWS + 2 * PAD
KW = 31
F32 = jnp.float32
BF16 = jnp.bfloat16
CHUNK = 256
VMEM = pl.BlockSpec(memory_space=pltpu.VMEM)


def group_mean(x, avg):
    high = x.astype(BF16)
    low = (x - high.astype(F32)).astype(BF16)
    return jnp.dot(high, avg, preferred_element_type=F32) + jnp.dot(
        low, avg, preferred_element_type=F32
    )


def averaging():
    rows = lax.broadcasted_iota(jnp.int32, (CH, CH), 0) // GROUP
    cols = lax.broadcasted_iota(jnp.int32, (CH, CH), 1) // GROUP
    return jnp.where(rows == cols, 1.0 / GROUP, 0.0).astype(BF16)


def convolve(src, taps_at, store):
    tiles = 8
    for block in range(CH // LANES):

        def some_rows(step, _, block=block):
            start = pl.multiple_of(step * (8 * tiles), 8 * tiles)
            sums = [None] * tiles
            for k in range(KW):
                tap = taps_at(k, block)
                for j in range(tiles):
                    part = src[block, pl.ds(start + 8 * j + k + 1, 8), :] * tap
                    sums[j] = part if sums[j] is None else sums[j] + part
            for j in range(tiles):
                store(block, pl.multiple_of(start + 8 * j, 8), sums[j])
            return 0

        lax.fori_loop(0, ROWS // (8 * tiles), some_rows, 0)


def is_second():
    return lax.axis_index("c") == 1


def sides(second, inner, outer):
    return jnp.where(second, inner, outer), jnp.where(second, outer, inner)


def neighbours(inner, outer):
    second = is_second()
    before = jnp.where(second, inner[PAD : 2 * PAD].astype(F32), outer[PAD : 2 * PAD].astype(F32))
    after = jnp.where(second, outer[0:PAD].astype(F32), inner[0:PAD].astype(F32))
    return before, after


def edge_kernel(value_head, gate_head, value_tail, gate_tail, edges):
    def gated(value, gate):
        return (value[...].astype(F32) * jax.nn.sigmoid(gate[...].astype(F32))).astype(BF16)

    edges[0:PAD, :] = gated(value_head, gate_head)
    edges[PAD : 2 * PAD, :] = gated(value_tail, gate_tail)


def forward_kernel(
    value, gate, inner, outer, taps, gain, wide, unit, inv, slope, normed, conv
):
    lanes = [slice(b * LANES, (b + 1) * LANES) for b in range(2)]
    before, after = neighbours(inner, outer)
    for b in range(2):
        wide[b, 0:PAD, :] = before[:, lanes[b]]
        wide[b, PAD + ROWS : HALO, :] = after[:, lanes[b]]

    def gate_rows(step, _):
        start = pl.multiple_of(step * 64, 64)
        rows = pl.ds(start, 64)
        gated = (value[rows, :].astype(F32) * jax.nn.sigmoid(gate[rows, :].astype(F32))).astype(
            BF16
        )
        for b in range(2):
            wide[b, pl.ds(pl.multiple_of(start + PAD, 16), 64), :] = gated[:, lanes[b]].astype(F32)
        return 0

    lax.fori_loop(0, ROWS // 64, gate_rows, 0)

    def store(block, start, rows):
        conv[pl.ds(start, 8), lanes[block]] = rows

    lines = taps[...].astype(F32)
    convolve(
        wide, lambda k, b: jnp.broadcast_to(lines[k : k + 1, lanes[b]], (8, LANES)), store
    )
    avg = averaging()
    gain_row = gain[...]

    def norm_rows(step, _):
        rows = pl.ds(pl.multiple_of(step * CHUNK, CHUNK), CHUNK)
        raw = conv[rows, :]
        centred = raw - group_mean(raw, avg)
        scale = lax.rsqrt(group_mean(centred * centred, avg) + EPS)
        unit_rows = centred * scale
        pre = unit_rows * gain_row
        s = jax.nn.sigmoid(pre)
        unit[rows, :] = unit_rows
        inv[rows, :] = scale
        slope[rows, :] = s * (1.0 + pre * (1.0 - s))
        normed[rows, :] = (pre * s).astype(BF16)
        return 0

    lax.fori_loop(0, ROWS // CHUNK, norm_rows, 0)


def homes(y):
    return y, lax.bitwise_xor(y, 1), 3 - y, lax.bitwise_xor(y, 2)


def early_kernel(own, left, right, weight, normed, partial, wgrad):
    y = lax.axis_index("tp")
    blocks = tuple(zip((own, left, right), homes(y)))
    weights = [weight[pl.ds(pl.multiple_of(at * CH, CH), CH), :] for _, at in blocks]

    def some_rows(step, _):
        rows = pl.ds(pl.multiple_of(step * CHUNK, CHUNK), CHUNK)
        total = None
        for (ref, _), w in zip(blocks, weights):
            part = jnp.dot(ref[rows, :], w, preferred_element_type=F32)
            total = part if total is None else total + part
        partial[rows, :] = total
        return 0

    lax.fori_loop(0, ROWS // CHUNK, some_rows, 0)
    for d, (ref, _) in enumerate(blocks):
        grads = lax.dot_general(
            ref[...], normed[...], (((0,), (0,)), ((), ())), preferred_element_type=F32
        )
        pieces = grads.reshape(4, 8, 8, CH).astype(BF16)
        for near in range(4):
            wgrad[:, d * 4 + near] = pieces[near]


def late_kernel(
    far_top, far_bottom, weight, normed, partial, unit, inv, slope, gain, wide, begun, grad, ends, sums
):
    y = lax.axis_index("tp")
    w = weight[pl.ds(pl.multiple_of(homes(y)[3] * CH, CH), CH), :]
    avg = averaging()
    gain_row = gain[...]

    def some_rows(step, gain_sum, far, base):
        start = pl.multiple_of(step * CHUNK, CHUNK)
        rows = pl.ds(start + base, CHUNK)
        normed_grad = partial[rows, :] + jnp.dot(
            far[pl.ds(start, CHUNK), :], w, preferred_element_type=F32)
        u = unit[rows, :]
        act = normed_grad * slope[rows, :]
        au = act * u
        hat = act * gain_row
        hat_unit = au * gain_row
        rows_grad = inv[rows, :] * (
            hat - group_mean(hat, avg) - u * group_mean(hat_unit, avg)
        )
        for b in range(2):
            grad[b, rows, :] = rows_grad[:, b * LANES : (b + 1) * LANES]
        return gain_sum + jnp.sum(au.reshape(CHUNK // 8, 8, CH), axis=0)

    gain_sum = jnp.zeros((8, CH), F32)
    for far, base in ((far_top, 0), (far_bottom, HALF)):
        gain_sum = lax.fori_loop(
            0, HALF // CHUNK, functools.partial(some_rows, far=far, base=base), gain_sum
        )
    for b in range(2):
        cols = slice(b * LANES, (b + 1) * LANES)
        ends[0:PAD, cols] = grad[b, 0:PAD, :]
        ends[PAD : 2 * PAD, cols] = grad[b, ROWS - PAD : ROWS, :]

    sums[:, 0:12] = begun[...]
    pieces = lax.dot_general(
        far_top[...], normed[0:HALF, :], (((0,), (0,)), ((), ())), preferred_element_type=F32
    ) + lax.dot_general(
        far_bottom[...], normed[HALF:ROWS, :], (((0,), (0,)), ((), ())), preferred_element_type=F32
    )
    pieces = pieces.reshape(4, 8, 8, CH).astype(BF16)
    for near in range(4):
        sums[:, 12 + near] = pieces[near]

    halves = []
    for b in range(2):
        lines = []
        for group in (range(0, 16), range(16, KW)):

            def tiles(step, carry, b=b, group=group):
                accs = list(carry)
                for j in range(4):
                    start = pl.multiple_of(step * 32, 32) + 8 * j
                    g = grad[b, pl.ds(start, 8), :]
                    for i, k in enumerate(group):
                        accs[i] = accs[i] + g * wide[b, pl.ds(start + k + 1, 8), :]
                return tuple(accs)

            accs = lax.fori_loop(
                0, ROWS // 32, tiles, tuple(jnp.zeros((8, LANES), F32) for _ in group)
            )
            lines += [jnp.sum(a, axis=0, keepdims=True) for a in accs]
        halves.append(jnp.concatenate(lines, axis=0))
    taps = jnp.concatenate(
        [
            jnp.concatenate(halves, axis=1),
            jnp.sum(gain_sum, axis=0, keepdims=True),
        ],
        axis=0,
    ).astype(BF16)
    for peer in range(8):
        for part in range(2):
            line = (peer % 2) * 16 + part * 8
            sums[peer, 16 + part] = taps[line : line + 8]


def backward_kernel(
    value, gate, grad, inner, outer, taps, value_grad, gate_grad, wide, conv
):
    before, after = neighbours(inner, outer)
    lines = taps[...].astype(F32)
    lanes = [slice(b * LANES, (b + 1) * LANES) for b in range(2)]
    for b in range(2):
        wide[b, 0:PAD, :] = before[:, lanes[b]]
        wide[b, PAD : PAD + ROWS, :] = grad[b]
        wide[b, PAD + ROWS : HALO, :] = after[:, lanes[b]]

    def store(block, start, rows):
        conv[pl.ds(start, 8), lanes[block]] = rows

    convolve(
        wide,
        lambda k, b: jnp.broadcast_to(lines[KW - 1 - k : KW - k, lanes[b]], (8, LANES)),
        store,
    )

    def finish(step, _):
        rows = pl.ds(pl.multiple_of(step * 64, 64), 64)
        s = jax.nn.sigmoid(gate[rows, :].astype(F32))
        down = conv[rows, :] * s
        value_grad[rows, :] = down.astype(BF16)
        gate_grad[rows, :] = (down * value[rows, :].astype(F32) * (1.0 - s)).astype(BF16)
        return 0

    lax.fori_loop(0, ROWS // 64, finish, 0)


def middle_kernel(late, out):
    y = lax.axis_index("tp")

    def total(tile):
        sums = late[0, tile].astype(F32)
        for peer in range(1, 8):
            sums = sums + late[peer, tile].astype(F32)
        return sums.astype(BF16)

    taps = [total(16 + part) for part in range(2)]
    for d, home in enumerate(homes(y)):
        for near in range(4):
            out[home * 4 + near, 0] = total(d * 4 + near)
            for part in range(2):
                out[home * 4 + near, 1 + part] = taps[part]


def whole_kernel(got, weight, mine):
    total = got[0].astype(F32)
    for peer in range(1, 16):
        total = total + got[peer].astype(F32)
    weight[...] = total[0]
    mine[0:8] = total[1]
    mine[8:16] = total[2]


def last_kernel(mine, other, taps, gain):
    low, high = sides(is_second(), other[...], mine[...])
    taps[0:16] = low
    taps[16:31] = high[:15]
    gain[...] = high[15:16]


def call(kernel, outs, specs, scratch=(), cost=None):
    return pl.pallas_call(
        kernel,
        out_shape=outs,
        in_specs=specs,
        out_specs=jax.tree.map(lambda _: VMEM, outs),
        scratch_shapes=scratch,
        cost_estimate=cost,
        compiler_params=pltpu.CompilerParams(vmem_limit_bytes=8 * 1024 * 1024),
    )


def shape(*dims, dtype=F32):
    return jax.ShapeDtypeStruct(dims, dtype)


def cost(us):
    return pl.CostEstimate(flops=int(us * 1e-6 * 2e14), bytes_accessed=2**20, transcendentals=0)


def ring(size, by):
    return [(i, (i + by) % size) for i in range(size)]


def body(value_rows, gate_rows, conv_taps, norm_gain, point_weight, out_grad):
    peers = lax.axis_size(SP)
    pairs = [(i, i ^ 1) for i in range(peers)]
    apart = [(i, i + 1) for i in range(1, peers - 1, 2)]
    apart = apart + [(j, i) for i, j in apart]
    gain = norm_gain.reshape(1, CH)

    def exchange(array, axis):
        return lax.all_to_all(array, axis, 0, 0, tiled=True)

    first_rows = pl.BlockSpec((PAD, CH), lambda i: (0, 0))
    last_rows = pl.BlockSpec((PAD, CH), lambda i: (ROWS // PAD - 1, 0))
    edges = pl.pallas_call(
        edge_kernel,
        out_shape=shape(2 * PAD, CH, dtype=BF16),
        grid=(1,),
        in_specs=[first_rows, first_rows, last_rows, last_rows],
        out_specs=pl.BlockSpec((2 * PAD, CH), lambda i: (0, 0)),
        name="edges",
    )(value_rows, gate_rows, value_rows, gate_rows)
    beside = [(i, i ^ 1) for i in range(4)]
    around = [(i, 3 - i) for i in range(4)]
    left = lax.ppermute(out_grad, "tp", beside)
    right = lax.ppermute(out_grad, "tp", around)
    inner = lax.ppermute(edges, SP, pairs)
    outer = lax.ppermute(edges, SP, apart)
    far_top = lax.ppermute(left[:HALF], "tp", around)
    far_bottom = lax.ppermute(right[HALF:], "tp", beside)

    wide, unit, inv, slope, normed = call(
        forward_kernel,
        (
            shape(2, HALO, LANES),
            shape(ROWS, CH),
            shape(ROWS, CH),
            shape(ROWS, CH),
            shape(ROWS, CH, dtype=BF16),
        ),
        [VMEM] * 6,
        [pltpu.VMEM((ROWS, CH), F32)],
        cost(7),
    )(value_rows, gate_rows, inner, outer, conv_taps, gain)

    partial, wgrad = call(
        early_kernel, (shape(ROWS, CH), shape(8, 12, 8, CH, dtype=BF16)), [VMEM] * 5, (), cost(4)
    )(out_grad, left, right, point_weight, normed)

    grad, ends, sums = call(
        late_kernel,
        (
            shape(2, ROWS, LANES),
            shape(2 * PAD, CH),
            shape(8, 18, 8, CH, dtype=BF16),
        ),
        [VMEM] * 11,
        (),
        cost(8),
    )(far_top, far_bottom, point_weight, normed, partial, unit, inv, slope, gain, wide, wgrad)
    late = exchange(sums, ("x", "c"))

    sent = call(middle_kernel, shape(16, 3, 8, CH, dtype=BF16), [VMEM], (), cost(1))(late)
    got = exchange(sent, "z")

    inner = lax.ppermute(ends, SP, pairs)
    outer = lax.ppermute(ends, SP, apart)
    value_grad, gate_grad = call(
        backward_kernel,
        (shape(ROWS, CH, dtype=BF16), shape(ROWS, CH, dtype=BF16)),
        [VMEM] * 6,
        [pltpu.VMEM((2, HALO, LANES), F32), pltpu.VMEM((ROWS, CH), F32)],
        cost(6),
    )(value_rows, gate_rows, grad, inner, outer, conv_taps)

    got, value_grad, gate_grad = lax.optimization_barrier((got, value_grad, gate_grad))
    weight_grad, mine = call(whole_kernel, (shape(8, CH), shape(16, CH)), [VMEM], (), cost(1))(got)
    other = lax.ppermute(mine, "c", ring(2, 1))
    taps_grad, gain_grad = call(
        last_kernel, (shape(KW, CH), shape(1, CH)), [VMEM, VMEM], (), cost(1)
    )(mine, other)
    return value_grad, gate_grad, taps_grad, gain_grad.reshape(CH), weight_grad


def solution(mesh):
    finer = Mesh(mesh.devices.reshape(16, 4, 2, mesh.shape["tp"]), ("z", "x", "c", "tp"))
    return jax.shard_map(
        body,
        mesh=finer,
        in_specs=(P(SP, "tp"), P(SP, "tp"), P(None, "tp"), P("tp"), P(None, "tp"), P(SP, "tp")),
        out_specs=(P(SP, "tp"), P(SP, "tp"), P(None, "tp"), P("tp"), P(SP, "tp")),
        check_vma=False,
    )
```

```python
import functools

import jax
import jax.numpy as jnp
from jax import lax
from jax.experimental import pallas as pl
from jax.experimental.pallas import tpu as pltpu
from jax.sharding import Mesh
from jax.sharding import PartitionSpec as P


GROUP = 64
SP = ("z", "x", "c")
EPS = 1e-06
ROWS = 1024
CH = 256
LANES = 128
HALF = 512
PAD = 16
HALO = ROWS + 2 * PAD
KW = 31
F32 = jnp.float32
BF16 = jnp.bfloat16
CHUNK = 256
VMEM = pl.BlockSpec(memory_space=pltpu.VMEM)


def group_mean(x, avg):
    high = x.astype(BF16)
    low = (x - high.astype(F32)).astype(BF16)
    return jnp.dot(high, avg, preferred_element_type=F32) + jnp.dot(
        low, avg, preferred_element_type=F32
    )


def averaging():
    rows = lax.broadcasted_iota(jnp.int32, (CH, CH), 0) // GROUP
    cols = lax.broadcasted_iota(jnp.int32, (CH, CH), 1) // GROUP
    return jnp.where(rows == cols, 1.0 / GROUP, 0.0).astype(BF16)


def convolve(src, taps_at, store):
    tiles = 8
    for block in range(CH // LANES):

        def some_rows(step, _, block=block):
            start = pl.multiple_of(step * (8 * tiles), 8 * tiles)
            sums = [None] * tiles
            for k in range(KW):
                tap = taps_at(k, block)
                for j in range(tiles):
                    part = src[block, pl.ds(start + 8 * j + k + 1, 8), :] * tap
                    sums[j] = part if sums[j] is None else sums[j] + part
            for j in range(tiles):
                store(block, pl.multiple_of(start + 8 * j, 8), sums[j])
            return 0

        lax.fori_loop(0, ROWS // (8 * tiles), some_rows, 0)


def is_second():
    return lax.axis_index("c") == 1


def sides(second, inner, outer):
    return jnp.where(second, inner, outer), jnp.where(second, outer, inner)


def neighbours(inner, outer):
    second = is_second()
    before = jnp.where(second, inner[PAD : 2 * PAD].astype(F32), outer[PAD : 2 * PAD].astype(F32))
    after = jnp.where(second, outer[0:PAD].astype(F32), inner[0:PAD].astype(F32))
    return before, after


def edge_kernel(value_head, gate_head, value_tail, gate_tail, edges):
    def gated(value, gate):
        return (value[...].astype(F32) * jax.nn.sigmoid(gate[...].astype(F32))).astype(BF16)

    edges[0:PAD, :] = gated(value_head, gate_head)
    edges[PAD : 2 * PAD, :] = gated(value_tail, gate_tail)


def prepare_kernel(value, gate, taps, wide, conv):
    lanes = [slice(b * LANES, (b + 1) * LANES) for b in range(2)]
    for b in range(2):
        wide[b, 0:PAD, :] = jnp.zeros((PAD, LANES), F32)
        wide[b, PAD + ROWS : HALO, :] = jnp.zeros((PAD, LANES), F32)

    def gate_rows(step, _):
        start = pl.multiple_of(step * 64, 64)
        rows = pl.ds(start, 64)
        gated = (value[rows, :].astype(F32) * jax.nn.sigmoid(gate[rows, :].astype(F32))).astype(
            BF16
        )
        for b in range(2):
            wide[b, pl.ds(pl.multiple_of(start + PAD, 16), 64), :] = gated[:, lanes[b]].astype(F32)
        return 0

    lax.fori_loop(0, ROWS // 64, gate_rows, 0)

    def store(block, start, rows):
        conv[pl.ds(start, 8), lanes[block]] = rows

    lines = taps[...].astype(F32)
    convolve(
        wide, lambda k, b: jnp.broadcast_to(lines[k : k + 1, lanes[b]], (8, LANES)), store
    )


def forward_kernel(inner, outer, taps, gain, plain, conv, wide, unit, inv, slope, normed, fixed):
    lanes = [slice(b * LANES, (b + 1) * LANES) for b in range(2)]
    lines = taps[...].astype(F32)
    before, after = neighbours(inner, outer)
    for b in range(2):
        wide[b, 0:PAD, :] = before[:, lanes[b]]
        wide[b, PAD : PAD + ROWS, :] = plain[b, PAD : PAD + ROWS, :]
        wide[b, PAD + ROWS : HALO, :] = after[:, lanes[b]]
        for at, start in enumerate((0, 8, ROWS - 16, ROWS - 8)):
            total = None
            for k in range(KW):
                part = wide[b, start + k + 1 : start + k + 9, :] * lines[k : k + 1, lanes[b]]
                total = part if total is None else total + part
            fixed[at * 8 : at * 8 + 8, lanes[b]] = total
    avg = averaging()
    gain_row = gain[...]

    def norm_rows(start, raw):
        rows = pl.ds(start, CHUNK)
        centred = raw - group_mean(raw, avg)
        scale = lax.rsqrt(group_mean(centred * centred, avg) + EPS)
        unit_rows = centred * scale
        pre = unit_rows * gain_row
        s = jax.nn.sigmoid(pre)
        unit[rows, :] = unit_rows
        inv[rows, :] = scale
        slope[rows, :] = s * (1.0 + pre * (1.0 - s))
        normed[rows, :] = (pre * s).astype(BF16)

    def middle_rows(step, _):
        start = pl.multiple_of(step * CHUNK, CHUNK)
        norm_rows(start, conv[pl.ds(start, CHUNK), :])
        return 0

    norm_rows(0, jnp.concatenate([fixed[0:16, :], conv[16:CHUNK, :]], axis=0))
    lax.fori_loop(1, ROWS // CHUNK - 1, middle_rows, 0)
    last = ROWS - CHUNK
    norm_rows(last, jnp.concatenate([conv[last : ROWS - 16, :], fixed[16:32, :]], axis=0))


def homes(y):
    return y, lax.bitwise_xor(y, 1), 3 - y, lax.bitwise_xor(y, 2)


def early_kernel(own, left, right, weight, normed, partial, wgrad):
    y = lax.axis_index("tp")
    blocks = tuple(zip((own, left, right), homes(y)))
    weights = [weight[pl.ds(pl.multiple_of(at * CH, CH), CH), :] for _, at in blocks]

    def some_rows(step, _):
        rows = pl.ds(pl.multiple_of(step * CHUNK, CHUNK), CHUNK)
        total = None
        for (ref, _), w in zip(blocks, weights):
            part = jnp.dot(ref[rows, :], w, preferred_element_type=F32)
            total = part if total is None else total + part
        partial[rows, :] = total
        return 0

    lax.fori_loop(0, ROWS // CHUNK, some_rows, 0)
    for d, (ref, _) in enumerate(blocks):
        grads = lax.dot_general(
            ref[...], normed[...], (((0,), (0,)), ((), ())), preferred_element_type=F32
        )
        pieces = grads.reshape(4, 8, 8, CH).astype(BF16)
        for near in range(4):
            wgrad[:, d * 4 + near] = pieces[near]


def late_kernel(
    far_top, far_bottom, weight, normed, partial, unit, inv, slope, gain, wide, begun, grad, ends, sums
):
    y = lax.axis_index("tp")
    w = weight[pl.ds(pl.multiple_of(homes(y)[3] * CH, CH), CH), :]
    avg = averaging()
    gain_row = gain[...]

    def some_rows(step, gain_sum, far, base):
        start = pl.multiple_of(step * CHUNK, CHUNK)
        rows = pl.ds(start + base, CHUNK)
        normed_grad = partial[rows, :] + jnp.dot(
            far[pl.ds(start, CHUNK), :], w, preferred_element_type=F32)
        u = unit[rows, :]
        act = normed_grad * slope[rows, :]
        au = act * u
        hat = act * gain_row
        hat_unit = au * gain_row
        rows_grad = inv[rows, :] * (
            hat - group_mean(hat, avg) - u * group_mean(hat_unit, avg)
        )
        for b in range(2):
            grad[b, rows, :] = rows_grad[:, b * LANES : (b + 1) * LANES]
        return gain_sum + jnp.sum(au.reshape(CHUNK // 8, 8, CH), axis=0)

    gain_sum = jnp.zeros((8, CH), F32)
    for far, base in ((far_top, 0), (far_bottom, HALF)):
        gain_sum = lax.fori_loop(
            0, HALF // CHUNK, functools.partial(some_rows, far=far, base=base), gain_sum
        )
    for b in range(2):
        cols = slice(b * LANES, (b + 1) * LANES)
        ends[0:PAD, cols] = grad[b, 0:PAD, :]
        ends[PAD : 2 * PAD, cols] = grad[b, ROWS - PAD : ROWS, :]

    sums[:, 0:12] = begun[...]
    pieces = lax.dot_general(
        far_top[...], normed[0:HALF, :], (((0,), (0,)), ((), ())), preferred_element_type=F32
    ) + lax.dot_general(
        far_bottom[...], normed[HALF:ROWS, :], (((0,), (0,)), ((), ())), preferred_element_type=F32
    )
    pieces = pieces.reshape(4, 8, 8, CH).astype(BF16)
    for near in range(4):
        sums[:, 12 + near] = pieces[near]

    halves = []
    for b in range(2):
        lines = []
        for group in (range(0, 16), range(16, KW)):

            def tiles(step, carry, b=b, group=group):
                accs = list(carry)
                for j in range(4):
                    start = pl.multiple_of(step * 32, 32) + 8 * j
                    g = grad[b, pl.ds(start, 8), :]
                    for i, k in enumerate(group):
                        accs[i] = accs[i] + g * wide[b, pl.ds(start + k + 1, 8), :]
                return tuple(accs)

            accs = lax.fori_loop(
                0, ROWS // 32, tiles, tuple(jnp.zeros((8, LANES), F32) for _ in group)
            )
            lines += [jnp.sum(a, axis=0, keepdims=True) for a in accs]
        halves.append(jnp.concatenate(lines, axis=0))
    taps = jnp.concatenate(
        [
            jnp.concatenate(halves, axis=1),
            jnp.sum(gain_sum, axis=0, keepdims=True),
        ],
        axis=0,
    ).astype(BF16)
    for peer in range(8):
        for part in range(2):
            line = (peer % 2) * 16 + part * 8
            sums[peer, 16 + part] = taps[line : line + 8]


def backward_kernel(
    value, gate, grad, inner, outer, taps, value_grad, gate_grad, wide, conv
):
    before, after = neighbours(inner, outer)
    lines = taps[...].astype(F32)
    lanes = [slice(b * LANES, (b + 1) * LANES) for b in range(2)]
    for b in range(2):
        wide[b, 0:PAD, :] = before[:, lanes[b]]
        wide[b, PAD : PAD + ROWS, :] = grad[b]
        wide[b, PAD + ROWS : HALO, :] = after[:, lanes[b]]

    def store(block, start, rows):
        conv[pl.ds(start, 8), lanes[block]] = rows

    convolve(
        wide,
        lambda k, b: jnp.broadcast_to(lines[KW - 1 - k : KW - k, lanes[b]], (8, LANES)),
        store,
    )

    def finish(step, _):
        rows = pl.ds(pl.multiple_of(step * 64, 64), 64)
        s = jax.nn.sigmoid(gate[rows, :].astype(F32))
        down = conv[rows, :] * s
        value_grad[rows, :] = down.astype(BF16)
        gate_grad[rows, :] = (down * value[rows, :].astype(F32) * (1.0 - s)).astype(BF16)
        return 0

    lax.fori_loop(0, ROWS // 64, finish, 0)


def middle_kernel(late, out):
    y = lax.axis_index("tp")

    def total(tile):
        sums = late[0, tile].astype(F32)
        for peer in range(1, 8):
            sums = sums + late[peer, tile].astype(F32)
        return sums.astype(BF16)

    taps = [total(16 + part) for part in range(2)]
    for d, home in enumerate(homes(y)):
        for near in range(4):
            out[home * 4 + near, 0] = total(d * 4 + near)
            for part in range(2):
                out[home * 4 + near, 1 + part] = taps[part]


def whole_kernel(got, weight, mine):
    total = got[0].astype(F32)
    for peer in range(1, 16):
        total = total + got[peer].astype(F32)
    weight[...] = total[0]
    mine[0:8] = total[1]
    mine[8:16] = total[2]


def last_kernel(mine, other, taps, gain):
    low, high = sides(is_second(), other[...], mine[...])
    taps[0:16] = low
    taps[16:31] = high[:15]
    gain[...] = high[15:16]


def call(kernel, outs, specs, scratch=(), cost=None):
    return pl.pallas_call(
        kernel,
        out_shape=outs,
        in_specs=specs,
        out_specs=jax.tree.map(lambda _: VMEM, outs),
        scratch_shapes=scratch,
        cost_estimate=cost,
        compiler_params=pltpu.CompilerParams(vmem_limit_bytes=8 * 1024 * 1024),
    )


def shape(*dims, dtype=F32):
    return jax.ShapeDtypeStruct(dims, dtype)


def cost(us):
    return pl.CostEstimate(flops=int(us * 1e-6 * 2e14), bytes_accessed=2**20, transcendentals=0)


def ring(size, by):
    return [(i, (i + by) % size) for i in range(size)]


def body(value_rows, gate_rows, conv_taps, norm_gain, point_weight, out_grad):
    peers = lax.axis_size(SP)
    pairs = [(i, i ^ 1) for i in range(peers)]
    apart = [(i, i + 1) for i in range(1, peers - 1, 2)]
    apart = apart + [(j, i) for i, j in apart]
    gain = norm_gain.reshape(1, CH)

    def exchange(array, axis):
        return lax.all_to_all(array, axis, 0, 0, tiled=True)

    first_rows = pl.BlockSpec((PAD, CH), lambda i: (0, 0))
    last_rows = pl.BlockSpec((PAD, CH), lambda i: (ROWS // PAD - 1, 0))
    edges = pl.pallas_call(
        edge_kernel,
        out_shape=shape(2 * PAD, CH, dtype=BF16),
        grid=(1,),
        in_specs=[first_rows, first_rows, last_rows, last_rows],
        out_specs=pl.BlockSpec((2 * PAD, CH), lambda i: (0, 0)),
        name="edges",
    )(value_rows, gate_rows, value_rows, gate_rows)
    beside = [(i, i ^ 1) for i in range(4)]
    around = [(i, 3 - i) for i in range(4)]
    left = lax.ppermute(out_grad, "tp", beside)
    right = lax.ppermute(out_grad, "tp", around)
    inner = lax.ppermute(edges, SP, pairs)
    outer = lax.ppermute(edges, SP, apart)
    far_top = lax.ppermute(left[:HALF], "tp", around)
    far_bottom = lax.ppermute(right[HALF:], "tp", beside)

    plain, conv = call(
        prepare_kernel, (shape(2, HALO, LANES), shape(ROWS, CH)), [VMEM] * 3, (), cost(4)
    )(value_rows, gate_rows, conv_taps)
    wide, unit, inv, slope, normed = call(
        forward_kernel,
        (
            shape(2, HALO, LANES),
            shape(ROWS, CH),
            shape(ROWS, CH),
            shape(ROWS, CH),
            shape(ROWS, CH, dtype=BF16),
        ),
        [VMEM] * 6,
        [pltpu.VMEM((32, CH), F32)],
        cost(3),
    )(inner, outer, conv_taps, gain, plain, conv)

    partial, wgrad = call(
        early_kernel, (shape(ROWS, CH), shape(8, 12, 8, CH, dtype=BF16)), [VMEM] * 5, (), cost(4)
    )(out_grad, left, right, point_weight, normed)

    grad, ends, sums = call(
        late_kernel,
        (
            shape(2, ROWS, LANES),
            shape(2 * PAD, CH),
            shape(8, 18, 8, CH, dtype=BF16),
        ),
        [VMEM] * 11,
        (),
        cost(8),
    )(far_top, far_bottom, point_weight, normed, partial, unit, inv, slope, gain, wide, wgrad)
    late = exchange(sums, ("x", "c"))

    sent = call(middle_kernel, shape(16, 3, 8, CH, dtype=BF16), [VMEM], (), cost(1))(late)
    got = exchange(sent, "z")

    inner = lax.ppermute(ends, SP, pairs)
    outer = lax.ppermute(ends, SP, apart)
    value_grad, gate_grad = call(
        backward_kernel,
        (shape(ROWS, CH, dtype=BF16), shape(ROWS, CH, dtype=BF16)),
        [VMEM] * 6,
        [pltpu.VMEM((2, HALO, LANES), F32), pltpu.VMEM((ROWS, CH), F32)],
        cost(6),
    )(value_rows, gate_rows, grad, inner, outer, conv_taps)

    got, value_grad, gate_grad = lax.optimization_barrier((got, value_grad, gate_grad))
    weight_grad, mine = call(whole_kernel, (shape(8, CH), shape(16, CH)), [VMEM], (), cost(1))(got)
    other = lax.ppermute(mine, "c", ring(2, 1))
    taps_grad, gain_grad = call(
        last_kernel, (shape(KW, CH), shape(1, CH)), [VMEM, VMEM], (), cost(1)
    )(mine, other)
    return value_grad, gate_grad, taps_grad, gain_grad.reshape(CH), weight_grad


def solution(mesh):
    finer = Mesh(mesh.devices.reshape(16, 4, 2, mesh.shape["tp"]), ("z", "x", "c", "tp"))
    return jax.shard_map(
        body,
        mesh=finer,
        in_specs=(P(SP, "tp"), P(SP, "tp"), P(None, "tp"), P("tp"), P(None, "tp"), P(SP, "tp")),
        out_specs=(P(SP, "tp"), P(SP, "tp"), P(None, "tp"), P("tp"), P(SP, "tp")),
        check_vma=False,
    )
```

```python
import functools

import jax
import jax.numpy as jnp
from jax import lax
from jax.experimental import pallas as pl
from jax.experimental.pallas import tpu as pltpu
from jax.sharding import Mesh
from jax.sharding import PartitionSpec as P


GROUP = 64
SP = ("z", "x", "c")
EPS = 1e-06
ROWS = 1024
CH = 256
LANES = 128
HALF = 512
PAD = 16
HALO = ROWS + 2 * PAD
KW = 31
F32 = jnp.float32
BF16 = jnp.bfloat16
CHUNK = 256
VMEM = pl.BlockSpec(memory_space=pltpu.VMEM)


def group_mean(x, avg):
    high = x.astype(BF16)
    low = (x - high.astype(F32)).astype(BF16)
    return jnp.dot(high, avg, preferred_element_type=F32) + jnp.dot(
        low, avg, preferred_element_type=F32
    )


def averaging():
    rows = lax.broadcasted_iota(jnp.int32, (CH, CH), 0) // GROUP
    cols = lax.broadcasted_iota(jnp.int32, (CH, CH), 1) // GROUP
    return jnp.where(rows == cols, 1.0 / GROUP, 0.0).astype(BF16)


def convolve(src, taps_at, store):
    tiles = 8
    for block in range(CH // LANES):

        def some_rows(step, _, block=block):
            start = pl.multiple_of(step * (8 * tiles), 8 * tiles)
            sums = [None] * tiles
            for k in range(KW):
                tap = taps_at(k, block)
                for j in range(tiles):
                    part = src[block, pl.ds(start + 8 * j + k + 1, 8), :] * tap
                    sums[j] = part if sums[j] is None else sums[j] + part
            for j in range(tiles):
                store(block, pl.multiple_of(start + 8 * j, 8), sums[j])
            return 0

        lax.fori_loop(0, ROWS // (8 * tiles), some_rows, 0)


def is_second():
    return lax.axis_index("c") == 1


def sides(second, inner, outer):
    return jnp.where(second, inner, outer), jnp.where(second, outer, inner)


def neighbours(inner, outer):
    second = is_second()
    before = jnp.where(second, inner[PAD : 2 * PAD].astype(F32), outer[PAD : 2 * PAD].astype(F32))
    after = jnp.where(second, outer[0:PAD].astype(F32), inner[0:PAD].astype(F32))
    return before, after


def edge_kernel(value_head, gate_head, value_tail, gate_tail, edges):
    def gated(value, gate):
        return (value[...].astype(F32) * jax.nn.sigmoid(gate[...].astype(F32))).astype(BF16)

    edges[0:PAD, :] = gated(value_head, gate_head)
    edges[PAD : 2 * PAD, :] = gated(value_tail, gate_tail)


def prepare_kernel(value, gate, taps, wide, conv):
    lanes = [slice(b * LANES, (b + 1) * LANES) for b in range(2)]
    for b in range(2):
        wide[b, 0:PAD, :] = jnp.zeros((PAD, LANES), F32)
        wide[b, PAD + ROWS : HALO, :] = jnp.zeros((PAD, LANES), F32)

    def gate_rows(step, _):
        start = pl.multiple_of(step * 64, 64)
        rows = pl.ds(start, 64)
        gated = (value[rows, :].astype(F32) * jax.nn.sigmoid(gate[rows, :].astype(F32))).astype(
            BF16
        )
        for b in range(2):
            wide[b, pl.ds(pl.multiple_of(start + PAD, 16), 64), :] = gated[:, lanes[b]].astype(F32)
        return 0

    lax.fori_loop(0, ROWS // 64, gate_rows, 0)

    def store(block, start, rows):
        conv[pl.ds(start, 8), lanes[block]] = rows

    lines = taps[...].astype(F32)
    convolve(
        wide, lambda k, b: jnp.broadcast_to(lines[k : k + 1, lanes[b]], (8, LANES)), store
    )


def forward_kernel(inner, outer, taps, gain, plain, conv, wide, unit, inv, slope, normed, fixed):
    lanes = [slice(b * LANES, (b + 1) * LANES) for b in range(2)]
    lines = taps[...].astype(F32)
    before, after = neighbours(inner, outer)
    for b in range(2):
        wide[b, 0:PAD, :] = before[:, lanes[b]]
        wide[b, PAD : PAD + ROWS, :] = plain[b, PAD : PAD + ROWS, :]
        wide[b, PAD + ROWS : HALO, :] = after[:, lanes[b]]
        for at, start in enumerate((0, 8, ROWS - 16, ROWS - 8)):
            total = None
            for k in range(KW):
                part = wide[b, start + k + 1 : start + k + 9, :] * lines[k : k + 1, lanes[b]]
                total = part if total is None else total + part
            fixed[at * 8 : at * 8 + 8, lanes[b]] = total
    avg = averaging()
    gain_row = gain[...]

    def norm_rows(start, raw):
        rows = pl.ds(start, CHUNK)
        centred = raw - group_mean(raw, avg)
        scale = lax.rsqrt(group_mean(centred * centred, avg) + EPS)
        unit_rows = centred * scale
        pre = unit_rows * gain_row
        s = jax.nn.sigmoid(pre)
        unit[rows, :] = unit_rows
        inv[rows, :] = scale
        slope[rows, :] = s * (1.0 + pre * (1.0 - s))
        normed[rows, :] = (pre * s).astype(BF16)

    def middle_rows(step, _):
        start = pl.multiple_of(step * CHUNK, CHUNK)
        norm_rows(start, conv[pl.ds(start, CHUNK), :])
        return 0

    norm_rows(0, jnp.concatenate([fixed[0:16, :], conv[16:CHUNK, :]], axis=0))
    lax.fori_loop(1, ROWS // CHUNK - 1, middle_rows, 0)
    last = ROWS - CHUNK
    norm_rows(last, jnp.concatenate([conv[last : ROWS - 16, :], fixed[16:32, :]], axis=0))


def homes(y):
    return y, lax.bitwise_xor(y, 1), 3 - y, lax.bitwise_xor(y, 2)


def early_kernel(own, left, right, weight, normed, partial, kept, given):
    y = lax.axis_index("tp")
    blocks = tuple(zip((own, left, right), homes(y)))
    weights = [weight[pl.ds(pl.multiple_of(at * CH, CH), CH), :] for _, at in blocks]

    def some_rows(step, _):
        rows = pl.ds(pl.multiple_of(step * CHUNK, CHUNK), CHUNK)
        total = None
        for (ref, _), w in zip(blocks, weights):
            part = jnp.dot(ref[rows, :], w, preferred_element_type=F32)
            total = part if total is None else total + part
        partial[rows, :] = total
        return 0

    lax.fori_loop(0, ROWS // CHUNK, some_rows, 0)
    for d, (ref, _) in enumerate(blocks):
        grads = lax.dot_general(
            ref[...], normed[...], (((0,), (0,)), ((), ())), preferred_element_type=F32
        )
        pieces = grads.reshape(4, 8, 8, CH).astype(BF16)
        for m in range(2):
            even, odd = pieces[2 * m], pieces[2 * m + 1]
            kept[:, d * 2 + m], given[:, d * 2 + m] = sides(is_second(), odd, even)


def late_kernel(
    far_top, far_bottom, weight, normed, partial, unit, inv, slope, gain, wide, kept, taken, grad, ends, sums
):
    y = lax.axis_index("tp")
    w = weight[pl.ds(pl.multiple_of(homes(y)[3] * CH, CH), CH), :]
    avg = averaging()
    gain_row = gain[...]

    def some_rows(step, gain_sum, far, base):
        start = pl.multiple_of(step * CHUNK, CHUNK)
        rows = pl.ds(start + base, CHUNK)
        normed_grad = partial[rows, :] + jnp.dot(
            far[pl.ds(start, CHUNK), :], w, preferred_element_type=F32)
        u = unit[rows, :]
        act = normed_grad * slope[rows, :]
        au = act * u
        hat = act * gain_row
        hat_unit = au * gain_row
        rows_grad = inv[rows, :] * (
            hat - group_mean(hat, avg) - u * group_mean(hat_unit, avg)
        )
        for b in range(2):
            grad[b, rows, :] = rows_grad[:, b * LANES : (b + 1) * LANES]
        return gain_sum + jnp.sum(au.reshape(CHUNK // 8, 8, CH), axis=0)

    gain_sum = jnp.zeros((8, CH), F32)
    for far, base in ((far_top, 0), (far_bottom, HALF)):
        gain_sum = lax.fori_loop(
            0, HALF // CHUNK, functools.partial(some_rows, far=far, base=base), gain_sum
        )
    for b in range(2):
        cols = slice(b * LANES, (b + 1) * LANES)
        ends[0:PAD, cols] = grad[b, 0:PAD, :]
        ends[PAD : 2 * PAD, cols] = grad[b, ROWS - PAD : ROWS, :]

    sums[:, 0:6] = (kept[...].astype(F32) + taken[...].astype(F32)).astype(BF16)
    pieces = lax.dot_general(
        far_top[...], normed[0:HALF, :], (((0,), (0,)), ((), ())), preferred_element_type=F32
    ) + lax.dot_general(
        far_bottom[...], normed[HALF:ROWS, :], (((0,), (0,)), ((), ())), preferred_element_type=F32
    )
    pieces = pieces.reshape(4, 8, 8, CH).astype(BF16)
    for near in range(4):
        sums[:, 6 + near] = pieces[near]

    halves = []
    for b in range(2):
        lines = []
        for group in (range(0, 16), range(16, KW)):

            def tiles(step, carry, b=b, group=group):
                accs = list(carry)
                for j in range(4):
                    start = pl.multiple_of(step * 32, 32) + 8 * j
                    g = grad[b, pl.ds(start, 8), :]
                    for i, k in enumerate(group):
                        accs[i] = accs[i] + g * wide[b, pl.ds(start + k + 1, 8), :]
                return tuple(accs)

            accs = lax.fori_loop(
                0, ROWS // 32, tiles, tuple(jnp.zeros((8, LANES), F32) for _ in group)
            )
            lines += [jnp.sum(a, axis=0, keepdims=True) for a in accs]
        halves.append(jnp.concatenate(lines, axis=0))
    taps = jnp.concatenate(
        [
            jnp.concatenate(halves, axis=1),
            jnp.sum(gain_sum, axis=0, keepdims=True),
        ],
        axis=0,
    ).astype(BF16)
    for peer in range(8):
        for part in range(2):
            line = (peer % 2) * 16 + part * 8
            sums[peer, 10 + part] = taps[line : line + 8]


def backward_kernel(
    value, gate, grad, inner, outer, taps, value_grad, gate_grad, wide, conv
):
    before, after = neighbours(inner, outer)
    lines = taps[...].astype(F32)
    lanes = [slice(b * LANES, (b + 1) * LANES) for b in range(2)]
    for b in range(2):
        wide[b, 0:PAD, :] = before[:, lanes[b]]
        wide[b, PAD : PAD + ROWS, :] = grad[b]
        wide[b, PAD + ROWS : HALO, :] = after[:, lanes[b]]

    def store(block, start, rows):
        conv[pl.ds(start, 8), lanes[block]] = rows

    convolve(
        wide,
        lambda k, b: jnp.broadcast_to(lines[KW - 1 - k : KW - k, lanes[b]], (8, LANES)),
        store,
    )

    def finish(step, _):
        rows = pl.ds(pl.multiple_of(step * 64, 64), 64)
        s = jax.nn.sigmoid(gate[rows, :].astype(F32))
        down = conv[rows, :] * s
        value_grad[rows, :] = down.astype(BF16)
        gate_grad[rows, :] = (down * value[rows, :].astype(F32) * (1.0 - s)).astype(BF16)
        return 0

    lax.fori_loop(0, ROWS // 64, finish, 0)


def middle_kernel(late, out):
    y = lax.axis_index("tp")

    def total(tile, peers):
        sums = None
        for peer in peers:
            part = late[peer, tile].astype(F32)
            sums = part if sums is None else sums + part
        return sums.astype(BF16)

    taps = [total(10 + part, range(8)) for part in range(2)]
    for d, home in enumerate(homes(y)):
        for near in range(4):
            if d < 3:
                rows = total(d * 2 + near // 2, range(near % 2, 8, 2))
            else:
                rows = total(6 + near, range(8))
            out[home * 4 + near, 0] = rows
            for part in range(2):
                out[home * 4 + near, 1 + part] = taps[part]


def whole_kernel(got, weight, mine):
    total = got[0].astype(F32)
    for peer in range(1, 16):
        total = total + got[peer].astype(F32)
    weight[...] = total[0]
    mine[0:8] = total[1]
    mine[8:16] = total[2]


def last_kernel(mine, other, taps, gain):
    low, high = sides(is_second(), other[...], mine[...])
    taps[0:16] = low
    taps[16:31] = high[:15]
    gain[...] = high[15:16]


def call(kernel, outs, specs, scratch=(), cost=None):
    return pl.pallas_call(
        kernel,
        out_shape=outs,
        in_specs=specs,
        out_specs=jax.tree.map(lambda _: VMEM, outs),
        scratch_shapes=scratch,
        cost_estimate=cost,
        compiler_params=pltpu.CompilerParams(vmem_limit_bytes=8 * 1024 * 1024),
    )


def shape(*dims, dtype=F32):
    return jax.ShapeDtypeStruct(dims, dtype)


def cost(us):
    return pl.CostEstimate(flops=int(us * 1e-6 * 2e14), bytes_accessed=2**20, transcendentals=0)


def ring(size, by):
    return [(i, (i + by) % size) for i in range(size)]


def body(value_rows, gate_rows, conv_taps, norm_gain, point_weight, out_grad):
    peers = lax.axis_size(SP)
    pairs = [(i, i ^ 1) for i in range(peers)]
    apart = [(i, i + 1) for i in range(1, peers - 1, 2)]
    apart = apart + [(j, i) for i, j in apart]
    gain = norm_gain.reshape(1, CH)

    def exchange(array, axis):
        return lax.all_to_all(array, axis, 0, 0, tiled=True)

    first_rows = pl.BlockSpec((PAD, CH), lambda i: (0, 0))
    last_rows = pl.BlockSpec((PAD, CH), lambda i: (ROWS // PAD - 1, 0))
    edges = pl.pallas_call(
        edge_kernel,
        out_shape=shape(2 * PAD, CH, dtype=BF16),
        grid=(1,),
        in_specs=[first_rows, first_rows, last_rows, last_rows],
        out_specs=pl.BlockSpec((2 * PAD, CH), lambda i: (0, 0)),
        name="edges",
    )(value_rows, gate_rows, value_rows, gate_rows)
    beside = [(i, i ^ 1) for i in range(4)]
    around = [(i, 3 - i) for i in range(4)]
    left = lax.ppermute(out_grad, "tp", beside)
    right = lax.ppermute(out_grad, "tp", around)
    inner = lax.ppermute(edges, SP, pairs)
    outer = lax.ppermute(edges, SP, apart)
    far_top = lax.ppermute(left[:HALF], "tp", around)
    far_bottom = lax.ppermute(right[HALF:], "tp", beside)

    plain, conv = call(
        prepare_kernel, (shape(2, HALO, LANES), shape(ROWS, CH)), [VMEM] * 3, (), cost(4)
    )(value_rows, gate_rows, conv_taps)
    wide, unit, inv, slope, normed = call(
        forward_kernel,
        (
            shape(2, HALO, LANES),
            shape(ROWS, CH),
            shape(ROWS, CH),
            shape(ROWS, CH),
            shape(ROWS, CH, dtype=BF16),
        ),
        [VMEM] * 6,
        [pltpu.VMEM((32, CH), F32)],
        cost(3),
    )(inner, outer, conv_taps, gain, plain, conv)

    half = shape(8, 6, 8, CH, dtype=BF16)
    partial, kept, given = call(
        early_kernel, (shape(ROWS, CH), half, half), [VMEM] * 5, (), cost(4)
    )(out_grad, left, right, point_weight, normed)

    taken = lax.ppermute(given, SP, pairs)

    grad, ends, sums = call(
        late_kernel,
        (
            shape(2, ROWS, LANES),
            shape(2 * PAD, CH),
            shape(8, 12, 8, CH, dtype=BF16),
        ),
        [VMEM] * 12,
        (),
        cost(8),
    )(far_top, far_bottom, point_weight, normed, partial, unit, inv, slope, gain, wide, kept, taken)
    late = exchange(sums, ("x", "c"))

    sent = call(middle_kernel, shape(16, 3, 8, CH, dtype=BF16), [VMEM], (), cost(1))(late)
    got = exchange(sent, "z")

    inner = lax.ppermute(ends, SP, pairs)
    outer = lax.ppermute(ends, SP, apart)
    value_grad, gate_grad = call(
        backward_kernel,
        (shape(ROWS, CH, dtype=BF16), shape(ROWS, CH, dtype=BF16)),
        [VMEM] * 6,
        [pltpu.VMEM((2, HALO, LANES), F32), pltpu.VMEM((ROWS, CH), F32)],
        cost(6),
    )(value_rows, gate_rows, grad, inner, outer, conv_taps)

    got, value_grad, gate_grad = lax.optimization_barrier((got, value_grad, gate_grad))
    weight_grad, mine = call(whole_kernel, (shape(8, CH), shape(16, CH)), [VMEM], (), cost(1))(got)
    other = lax.ppermute(mine, "c", ring(2, 1))
    taps_grad, gain_grad = call(
        last_kernel, (shape(KW, CH), shape(1, CH)), [VMEM, VMEM], (), cost(1)
    )(mine, other)
    return value_grad, gate_grad, taps_grad, gain_grad.reshape(CH), weight_grad


def solution(mesh):
    finer = Mesh(mesh.devices.reshape(16, 4, 2, mesh.shape["tp"]), ("z", "x", "c", "tp"))
    return jax.shard_map(
        body,
        mesh=finer,
        in_specs=(P(SP, "tp"), P(SP, "tp"), P(None, "tp"), P("tp"), P(None, "tp"), P(SP, "tp")),
        out_specs=(P(SP, "tp"), P(SP, "tp"), P(None, "tp"), P("tp"), P(SP, "tp")),
        check_vma=False,
    )
```

```python
import functools

import jax
import jax.numpy as jnp
from jax import lax
from jax.experimental import pallas as pl
from jax.experimental.pallas import tpu as pltpu
from jax.sharding import Mesh
from jax.sharding import PartitionSpec as P


GROUP = 64
SP = ("z", "x", "c")
EPS = 1e-06
ROWS = 1024
CH = 256
LANES = 128
HALF = 512
PAD = 16
HALO = ROWS + 2 * PAD
KW = 31
F32 = jnp.float32
BF16 = jnp.bfloat16
CHUNK = 256
VMEM = pl.BlockSpec(memory_space=pltpu.VMEM)


def group_mean(x, avg):
    high = x.astype(BF16)
    low = (x - high.astype(F32)).astype(BF16)
    return jnp.dot(high, avg, preferred_element_type=F32) + jnp.dot(
        low, avg, preferred_element_type=F32
    )


def rounded_mean(x, avg):
    return jnp.dot(x.astype(BF16), avg, preferred_element_type=F32)


def averaging():
    rows = lax.broadcasted_iota(jnp.int32, (CH, CH), 0) // GROUP
    cols = lax.broadcasted_iota(jnp.int32, (CH, CH), 1) // GROUP
    return jnp.where(rows == cols, 1.0 / GROUP, 0.0).astype(BF16)


def convolve(src, taps_at, store):
    tiles = 8
    for block in range(CH // LANES):

        def some_rows(step, _, block=block):
            start = pl.multiple_of(step * (8 * tiles), 8 * tiles)
            sums = [None] * tiles
            for k in range(KW):
                tap = taps_at(k, block)
                for j in range(tiles):
                    part = src[block, pl.ds(start + 8 * j + k + 1, 8), :] * tap
                    sums[j] = part if sums[j] is None else sums[j] + part
            for j in range(tiles):
                store(block, pl.multiple_of(start + 8 * j, 8), sums[j])
            return 0

        lax.fori_loop(0, ROWS // (8 * tiles), some_rows, 0)


def is_second():
    return lax.axis_index("c") == 1


def sides(second, inner, outer):
    return jnp.where(second, inner, outer), jnp.where(second, outer, inner)


def neighbours(inner, outer):
    second = is_second()
    before = jnp.where(second, inner[PAD : 2 * PAD].astype(F32), outer[PAD : 2 * PAD].astype(F32))
    after = jnp.where(second, outer[0:PAD].astype(F32), inner[0:PAD].astype(F32))
    return before, after


def edge_kernel(value_head, gate_head, value_tail, gate_tail, edges):
    def gated(value, gate):
        return (value[...].astype(F32) * jax.nn.sigmoid(gate[...].astype(F32))).astype(BF16)

    edges[0:PAD, :] = gated(value_head, gate_head)
    edges[PAD : 2 * PAD, :] = gated(value_tail, gate_tail)


def prepare_kernel(value, gate, taps, wide, conv):
    lanes = [slice(b * LANES, (b + 1) * LANES) for b in range(2)]
    for b in range(2):
        wide[b, 0:PAD, :] = jnp.zeros((PAD, LANES), F32)
        wide[b, PAD + ROWS : HALO, :] = jnp.zeros((PAD, LANES), F32)

    def gate_rows(step, _):
        start = pl.multiple_of(step * 64, 64)
        rows = pl.ds(start, 64)
        gated = (value[rows, :].astype(F32) * jax.nn.sigmoid(gate[rows, :].astype(F32))).astype(
            BF16
        )
        for b in range(2):
            wide[b, pl.ds(pl.multiple_of(start + PAD, 16), 64), :] = gated[:, lanes[b]].astype(F32)
        return 0

    lax.fori_loop(0, ROWS // 64, gate_rows, 0)

    def store(block, start, rows):
        conv[pl.ds(start, 8), lanes[block]] = rows

    lines = taps[...].astype(F32)
    convolve(
        wide, lambda k, b: jnp.broadcast_to(lines[k : k + 1, lanes[b]], (8, LANES)), store
    )


def forward_kernel(inner, outer, taps, gain, plain, conv, wide, unit, inv, slope, normed, fixed):
    lanes = [slice(b * LANES, (b + 1) * LANES) for b in range(2)]
    lines = taps[...].astype(F32)
    before, after = neighbours(inner, outer)
    for b in range(2):
        wide[b, 0:PAD, :] = before[:, lanes[b]]
        wide[b, PAD : PAD + ROWS, :] = plain[b, PAD : PAD + ROWS, :]
        wide[b, PAD + ROWS : HALO, :] = after[:, lanes[b]]
        for at, start in enumerate((0, 8, ROWS - 16, ROWS - 8)):
            total = None
            for k in range(KW):
                part = wide[b, start + k + 1 : start + k + 9, :] * lines[k : k + 1, lanes[b]]
                total = part if total is None else total + part
            fixed[at * 8 : at * 8 + 8, lanes[b]] = total
    avg = averaging()
    gain_row = gain[...]

    def norm_rows(start, raw):
        rows = pl.ds(start, CHUNK)
        centred = raw - group_mean(raw, avg)
        scale = lax.rsqrt(rounded_mean(centred * centred, avg) + EPS)
        unit_rows = centred * scale
        pre = unit_rows * gain_row
        s = jax.nn.sigmoid(pre)
        unit[rows, :] = unit_rows
        inv[rows, :] = scale
        slope[rows, :] = s * (1.0 + pre * (1.0 - s))
        normed[rows, :] = (pre * s).astype(BF16)

    def middle_rows(step, _):
        start = pl.multiple_of(step * CHUNK, CHUNK)
        norm_rows(start, conv[pl.ds(start, CHUNK), :])
        return 0

    norm_rows(0, jnp.concatenate([fixed[0:16, :], conv[16:CHUNK, :]], axis=0))
    lax.fori_loop(1, ROWS // CHUNK - 1, middle_rows, 0)
    last = ROWS - CHUNK
    norm_rows(last, jnp.concatenate([conv[last : ROWS - 16, :], fixed[16:32, :]], axis=0))


def homes(y):
    return y, lax.bitwise_xor(y, 1), 3 - y, lax.bitwise_xor(y, 2)


def early_kernel(own, left, right, weight, normed, partial, kept, given):
    y = lax.axis_index("tp")
    blocks = tuple(zip((own, left, right), homes(y)))
    weights = [weight[pl.ds(pl.multiple_of(at * CH, CH), CH), :] for _, at in blocks]

    def some_rows(step, _):
        rows = pl.ds(pl.multiple_of(step * CHUNK, CHUNK), CHUNK)
        total = None
        for (ref, _), w in zip(blocks, weights):
            part = jnp.dot(ref[rows, :], w, preferred_element_type=F32)
            total = part if total is None else total + part
        partial[rows, :] = total
        return 0

    lax.fori_loop(0, ROWS // CHUNK, some_rows, 0)
    for d, (ref, _) in enumerate(blocks):
        grads = lax.dot_general(
            ref[...], normed[...], (((0,), (0,)), ((), ())), preferred_element_type=F32
        )
        pieces = grads.reshape(4, 8, 8, CH).astype(BF16)
        for m in range(2):
            even, odd = pieces[2 * m], pieces[2 * m + 1]
            kept[:, d * 2 + m], given[:, d * 2 + m] = sides(is_second(), odd, even)


def late_kernel(
    far_top, far_bottom, weight, normed, partial, unit, inv, slope, gain, wide, kept, taken, grad, ends, sums
):
    y = lax.axis_index("tp")
    w = weight[pl.ds(pl.multiple_of(homes(y)[3] * CH, CH), CH), :]
    avg = averaging()
    gain_row = gain[...]

    def some_rows(step, gain_sum, far, base):
        start = pl.multiple_of(step * CHUNK, CHUNK)
        rows = pl.ds(start + base, CHUNK)
        normed_grad = partial[rows, :] + jnp.dot(
            far[pl.ds(start, CHUNK), :], w, preferred_element_type=F32)
        u = unit[rows, :]
        act = normed_grad * slope[rows, :]
        au = act * u
        hat = act * gain_row
        hat_unit = au * gain_row
        rows_grad = inv[rows, :] * (
            hat - group_mean(hat, avg) - u * rounded_mean(hat_unit, avg)
        )
        for b in range(2):
            grad[b, rows, :] = rows_grad[:, b * LANES : (b + 1) * LANES]
        return gain_sum + jnp.sum(au.reshape(CHUNK // 8, 8, CH), axis=0)

    gain_sum = jnp.zeros((8, CH), F32)
    for far, base in ((far_top, 0), (far_bottom, HALF)):
        gain_sum = lax.fori_loop(
            0, HALF // CHUNK, functools.partial(some_rows, far=far, base=base), gain_sum
        )
    for b in range(2):
        cols = slice(b * LANES, (b + 1) * LANES)
        ends[0:PAD, cols] = grad[b, 0:PAD, :]
        ends[PAD : 2 * PAD, cols] = grad[b, ROWS - PAD : ROWS, :]

    sums[:, 0:6] = (kept[...].astype(F32) + taken[...].astype(F32)).astype(BF16)
    pieces = lax.dot_general(
        far_top[...], normed[0:HALF, :], (((0,), (0,)), ((), ())), preferred_element_type=F32
    ) + lax.dot_general(
        far_bottom[...], normed[HALF:ROWS, :], (((0,), (0,)), ((), ())), preferred_element_type=F32
    )
    pieces = pieces.reshape(4, 8, 8, CH).astype(BF16)
    for near in range(4):
        sums[:, 6 + near] = pieces[near]

    halves = []
    for b in range(2):
        lines = []
        for group in (range(0, 16), range(16, KW)):

            def tiles(step, carry, b=b, group=group):
                accs = list(carry)
                for j in range(4):
                    start = pl.multiple_of(step * 32, 32) + 8 * j
                    g = grad[b, pl.ds(start, 8), :]
                    for i, k in enumerate(group):
                        accs[i] = accs[i] + g * wide[b, pl.ds(start + k + 1, 8), :]
                return tuple(accs)

            accs = lax.fori_loop(
                0, ROWS // 32, tiles, tuple(jnp.zeros((8, LANES), F32) for _ in group)
            )
            lines += [jnp.sum(a, axis=0, keepdims=True) for a in accs]
        halves.append(jnp.concatenate(lines, axis=0))
    taps = jnp.concatenate(
        [
            jnp.concatenate(halves, axis=1),
            jnp.sum(gain_sum, axis=0, keepdims=True),
        ],
        axis=0,
    ).astype(BF16)
    for peer in range(8):
        for part in range(2):
            line = (peer % 2) * 16 + part * 8
            sums[peer, 10 + part] = taps[line : line + 8]


def backward_kernel(
    value, gate, grad, inner, outer, taps, value_grad, gate_grad, wide, conv
):
    before, after = neighbours(inner, outer)
    lines = taps[...].astype(F32)
    lanes = [slice(b * LANES, (b + 1) * LANES) for b in range(2)]
    for b in range(2):
        wide[b, 0:PAD, :] = before[:, lanes[b]]
        wide[b, PAD : PAD + ROWS, :] = grad[b]
        wide[b, PAD + ROWS : HALO, :] = after[:, lanes[b]]

    def store(block, start, rows):
        conv[pl.ds(start, 8), lanes[block]] = rows

    convolve(
        wide,
        lambda k, b: jnp.broadcast_to(lines[KW - 1 - k : KW - k, lanes[b]], (8, LANES)),
        store,
    )

    def finish(step, _):
        rows = pl.ds(pl.multiple_of(step * 64, 64), 64)
        s = jax.nn.sigmoid(gate[rows, :].astype(F32))
        down = conv[rows, :] * s
        value_grad[rows, :] = down.astype(BF16)
        gate_grad[rows, :] = (down * value[rows, :].astype(F32) * (1.0 - s)).astype(BF16)
        return 0

    lax.fori_loop(0, ROWS // 64, finish, 0)


def middle_kernel(late, out):
    y = lax.axis_index("tp")

    def total(tile, peers):
        sums = None
        for peer in peers:
            part = late[peer, tile].astype(F32)
            sums = part if sums is None else sums + part
        return sums.astype(BF16)

    taps = [total(10 + part, range(8)) for part in range(2)]
    for d, home in enumerate(homes(y)):
        for near in range(4):
            if d < 3:
                rows = total(d * 2 + near // 2, range(near % 2, 8, 2))
            else:
                rows = total(6 + near, range(8))
            out[home * 4 + near, 0] = rows
            for part in range(2):
                out[home * 4 + near, 1 + part] = taps[part]


def whole_kernel(got, weight, mine):
    total = got[0].astype(F32)
    for peer in range(1, 16):
        total = total + got[peer].astype(F32)
    weight[...] = total[0]
    mine[0:8] = total[1]
    mine[8:16] = total[2]


def last_kernel(mine, other, taps, gain):
    low, high = sides(is_second(), other[...], mine[...])
    taps[0:16] = low
    taps[16:31] = high[:15]
    gain[...] = high[15:16]


def call(kernel, outs, specs, scratch=(), cost=None):
    return pl.pallas_call(
        kernel,
        out_shape=outs,
        in_specs=specs,
        out_specs=jax.tree.map(lambda _: VMEM, outs),
        scratch_shapes=scratch,
        cost_estimate=cost,
        compiler_params=pltpu.CompilerParams(vmem_limit_bytes=8 * 1024 * 1024),
    )


def shape(*dims, dtype=F32):
    return jax.ShapeDtypeStruct(dims, dtype)


def cost(us):
    return pl.CostEstimate(flops=int(us * 1e-6 * 2e14), bytes_accessed=2**20, transcendentals=0)


def ring(size, by):
    return [(i, (i + by) % size) for i in range(size)]


def body(value_rows, gate_rows, conv_taps, norm_gain, point_weight, out_grad):
    peers = lax.axis_size(SP)
    pairs = [(i, i ^ 1) for i in range(peers)]
    apart = [(i, i + 1) for i in range(1, peers - 1, 2)]
    apart = apart + [(j, i) for i, j in apart]
    gain = norm_gain.reshape(1, CH)

    def exchange(array, axis):
        return lax.all_to_all(array, axis, 0, 0, tiled=True)

    first_rows = pl.BlockSpec((PAD, CH), lambda i: (0, 0))
    last_rows = pl.BlockSpec((PAD, CH), lambda i: (ROWS // PAD - 1, 0))
    edges = pl.pallas_call(
        edge_kernel,
        out_shape=shape(2 * PAD, CH, dtype=BF16),
        grid=(1,),
        in_specs=[first_rows, first_rows, last_rows, last_rows],
        out_specs=pl.BlockSpec((2 * PAD, CH), lambda i: (0, 0)),
        name="edges",
    )(value_rows, gate_rows, value_rows, gate_rows)
    beside = [(i, i ^ 1) for i in range(4)]
    around = [(i, 3 - i) for i in range(4)]
    left = lax.ppermute(out_grad, "tp", beside)
    right = lax.ppermute(out_grad, "tp", around)
    inner = lax.ppermute(edges, SP, pairs)
    outer = lax.ppermute(edges, SP, apart)
    far_top = lax.ppermute(left[:HALF], "tp", around)
    far_bottom = lax.ppermute(right[HALF:], "tp", beside)

    plain, conv = call(
        prepare_kernel, (shape(2, HALO, LANES), shape(ROWS, CH)), [VMEM] * 3, (), cost(4)
    )(value_rows, gate_rows, conv_taps)
    wide, unit, inv, slope, normed = call(
        forward_kernel,
        (
            shape(2, HALO, LANES),
            shape(ROWS, CH),
            shape(ROWS, CH),
            shape(ROWS, CH),
            shape(ROWS, CH, dtype=BF16),
        ),
        [VMEM] * 6,
        [pltpu.VMEM((32, CH), F32)],
        cost(3),
    )(inner, outer, conv_taps, gain, plain, conv)

    half = shape(8, 6, 8, CH, dtype=BF16)
    partial, kept, given = call(
        early_kernel, (shape(ROWS, CH), half, half), [VMEM] * 5, (), cost(4)
    )(out_grad, left, right, point_weight, normed)

    taken = lax.ppermute(given, SP, pairs)

    grad, ends, sums = call(
        late_kernel,
        (
            shape(2, ROWS, LANES),
            shape(2 * PAD, CH),
            shape(8, 12, 8, CH, dtype=BF16),
        ),
        [VMEM] * 12,
        (),
        cost(8),
    )(far_top, far_bottom, point_weight, normed, partial, unit, inv, slope, gain, wide, kept, taken)
    late = exchange(sums, ("x", "c"))

    sent = call(middle_kernel, shape(16, 3, 8, CH, dtype=BF16), [VMEM], (), cost(1))(late)
    got = exchange(sent, "z")

    inner = lax.ppermute(ends, SP, pairs)
    outer = lax.ppermute(ends, SP, apart)
    value_grad, gate_grad = call(
        backward_kernel,
        (shape(ROWS, CH, dtype=BF16), shape(ROWS, CH, dtype=BF16)),
        [VMEM] * 6,
        [pltpu.VMEM((2, HALO, LANES), F32), pltpu.VMEM((ROWS, CH), F32)],
        cost(6),
    )(value_rows, gate_rows, grad, inner, outer, conv_taps)

    got, value_grad, gate_grad = lax.optimization_barrier((got, value_grad, gate_grad))
    weight_grad, mine = call(whole_kernel, (shape(8, CH), shape(16, CH)), [VMEM], (), cost(1))(got)
    other = lax.ppermute(mine, "c", ring(2, 1))
    taps_grad, gain_grad = call(
        last_kernel, (shape(KW, CH), shape(1, CH)), [VMEM, VMEM], (), cost(1)
    )(mine, other)
    return value_grad, gate_grad, taps_grad, gain_grad.reshape(CH), weight_grad


def solution(mesh):
    finer = Mesh(mesh.devices.reshape(16, 4, 2, mesh.shape["tp"]), ("z", "x", "c", "tp"))
    return jax.shard_map(
        body,
        mesh=finer,
        in_specs=(P(SP, "tp"), P(SP, "tp"), P(None, "tp"), P("tp"), P(None, "tp"), P(SP, "tp")),
        out_specs=(P(SP, "tp"), P(SP, "tp"), P(None, "tp"), P("tp"), P(SP, "tp")),
        check_vma=False,
    )
```
